128 devices in a mesh: sp: 32 (over z, y, core), tp: 4 (over x).
Axes of the slice: x: 4, y: 4, z: 4, core: 2. Of those that a mesh axis runs over, the one named last changes fastest.
Arguments:
- residual: bfloat16 [12288, 2048], P('sp'), may hold values from -50 to 50
- queries_a: bfloat16 [12288, 512], P('sp', 'tp'), may hold values from -50 to 50
- keys_a: bfloat16 [12288, 512], P('sp', 'tp'), may hold values from -9 to 9
- values_a: bfloat16 [12288, 512], P('sp', 'tp'), may hold values from -6 to 6
- queries_b: bfloat16 [12288, 1024], P('sp', 'tp'), may hold values from -50 to 50
- keys_b: bfloat16 [12288, 1024], P('sp', 'tp'), may hold values from -9 to 9
- values_b: bfloat16 [12288, 512], P('sp', 'tp'), may hold values from -6 to 6
- mix_lambda: float32 [2, 4], P(None, 'tp'), may hold values from 0.3 to 0.8
- head_gain: float32 [2, 128], replicated, may hold values from 0.1 to 1.9
- out_a: bfloat16 [512, 2048], P('tp'), may hold values from -0.1875 to 0.1875
- out_b: bfloat16 [512, 2048], P('tp'), may hold values from -0.1875 to 0.1875
- norm_gain: float32 [2048], replicated, may hold values from 0.1 to 1.9
- w_gate: bfloat16 [2048, 5632], P('sp', 'tp'), may hold values from -0.125 to 0.125
- w_up: bfloat16 [2048, 5632], P('sp', 'tp'), may hold values from -0.125 to 0.125
- w_down: bfloat16 [5632, 2048], P('tp', 'sp'), may hold values from -0.21875 to 0.21875
Outputs:
- layer_out: bfloat16 [12288, 2048], P('sp', 'tp')
The draws below stay inside these ranges and needn't reach their ends.
All inputs are finite; a program needn't handle non-finite values.
Results may differ from the reference program's by a relative error of at most 0.0085.
Values may be sent and summed in bfloat16 or wider, within the bound.
A program may use at most 256 MiB of HBM per device.

```python
import math
import jax
import jax.numpy as jnp
from jax import lax

D = 2048
FF = 5632
HEADS = 4
QA = 64
QB = 128
VD = 128
TOKENS = 12288


def draw_residual(key, part):
    base = jax.random.fold_in(key, 3)
    first, second = jax.random.split(base, 2)
    column = jnp.arange(D, dtype=jnp.float32) / D
    noise = jnp.clip(jax.random.normal(first, (TOKENS, D), jnp.float32), -6.0, 6.0)
    columns = 0.4 * 10.0 ** column
    row_scale = 2.0 ** jax.random.uniform(second, (TOKENS, 1), jnp.float32, -1.0, 1.0)
    return (noise * columns[None, :] * row_scale).astype(jnp.bfloat16)


def paired(key, width, salt):
    base = jax.random.fold_in(key, salt)
    query_seed, key_seed = jax.random.split(base, 2)
    columns = HEADS * 2 * width
    queries = 1.3 * jnp.clip(jax.random.normal(query_seed, (TOKENS, columns), jnp.float32), -6.0, 6.0)
    keys = 1.3 * jnp.clip(jax.random.normal(key_seed, (TOKENS, columns), jnp.float32), -6.0, 6.0)
    return (queries, keys)


def draw_queries_a(key, part):
    return paired(key, QA, 11)[0].astype(jnp.bfloat16)


def draw_keys_a(key, part):
    return paired(key, QA, 11)[1].astype(jnp.bfloat16)


def draw_queries_b(key, part):
    return paired(key, QB, 13)[0].astype(jnp.bfloat16)


def draw_keys_b(key, part):
    return paired(key, QB, 13)[1].astype(jnp.bfloat16)


def block_scale(rng, extent, pieces, least, largest):
    def one(position, blocks):
        draws = jax.random.uniform(jax.random.fold_in(jax.random.fold_in(rng, 6), position), (blocks,), jnp.float32, least / len(pieces), largest / len(pieces))
        return jnp.repeat(jnp.exp(draws), extent[position] // blocks).reshape((-1,) + (1,) * (len(extent) - position - 1))

    level = one(*pieces[0])
    for cut in pieces[1:]:
        level = level * one(*cut)
    return level


def scatter_about(key, shape, scale, limit, cuts=(), kind=jnp.bfloat16):
    level = block_scale(key, shape, cuts, -0.22, 0.18) if cuts else 1.0
    values = jax.random.normal(key, shape, jnp.float32) * scale * level
    return jnp.minimum(jnp.maximum(values, -limit), limit).astype(kind)


def setup_inputs(seed: int = 0) -> dict:
    streams_of = jax.random.split(jax.random.key(seed), 16)
    return {
        "residual": draw_residual(jax.random.fold_in(streams_of[15], 71), 0),
        "queries_a": draw_queries_a(jax.random.fold_in(streams_of[15], 71), 0),
        "keys_a": draw_keys_a(jax.random.fold_in(streams_of[15], 71), 0),
        "values_a": scatter_about(streams_of[3], (TOKENS, HEADS * VD), 1.0, 6.0, ((0, 32), (1, 4))),
        "queries_b": draw_queries_b(jax.random.fold_in(streams_of[15], 71), 0),
        "keys_b": draw_keys_b(jax.random.fold_in(streams_of[15], 71), 0),
        "values_b": scatter_about(streams_of[6], (TOKENS, HEADS * VD), 1.0, 6.0, ((0, 32), (1, 4))),
        "mix_lambda": jnp.clip(0.3 + 0.5 * jax.random.uniform(streams_of[7], (2, HEADS), jnp.float32) ** block_scale(streams_of[7], (2, HEADS), ((1, 4),), -0.2, 0.2), 0.3, 0.8),
        "head_gain": jnp.clip(1.0 + 0.18 * jax.random.normal(streams_of[8], (2, VD), jnp.float32), 0.1, 1.9),
        "out_a": scatter_about(streams_of[9], (HEADS * VD, D), (2 * HEADS * VD) ** -0.5, 0.1875, ((0, 4),)),
        "out_b": scatter_about(streams_of[10], (HEADS * VD, D), (2 * HEADS * VD) ** -0.5, 0.1875, ((0, 4),)),
        "norm_gain": jnp.clip(1.0 + 0.18 * jax.random.normal(streams_of[11], (D,), jnp.float32), 0.1, 1.9),
        "w_gate": scatter_about(streams_of[12], (D, FF), D ** -0.5, 0.125, ((0, 32), (1, 4))),
        "w_up": scatter_about(streams_of[13], (D, FF), D ** -0.5, 0.125, ((0, 32), (1, 4))),
        "w_down": scatter_about(streams_of[14], (FF, D), (FF // 8) ** -0.5, 0.21875, ((0, 4), (1, 32))),
    }


eps_norm = 1e-06
head_scale = 0.8

def group_attend(queries, keys, values, lambdas, gain, width):
    total = queries.shape[0]
    heads = lambdas.shape[0]
    block = math.gcd(total, 512)
    query_blocks = queries.reshape(total // block, block, heads, 2, width)
    key_rows = keys.reshape(total, heads, 2, width).astype(jnp.float32)
    value_rows = values.reshape(total, heads, values.shape[1] // heads).astype(jnp.float32)

    def one_block(query_block):
        scores = jnp.einsum('qhme,khme->mhqk', query_block.astype(jnp.float32), key_rows) * width ** (-0.5)
        peak = lax.optimization_barrier(jnp.max(scores, axis=-1, keepdims=True))
        weights = jnp.exp(scores - peak)
        denom = lax.optimization_barrier(jnp.sum(weights, axis=-1))
        rounded = lax.optimization_barrier(weights.astype(jnp.bfloat16)).astype(jnp.float32)
        numer = jnp.einsum('mhqk,khv->mhqv', rounded, value_rows)
        ratio = numer / denom[..., None]
        mixed = ratio[0] - lambdas[:, None, None] * ratio[1]
        inverse = lax.rsqrt(lax.optimization_barrier(jnp.mean(mixed * mixed, axis=-1, keepdims=True)) + eps_norm)
        normed = mixed * inverse * gain * head_scale
        return jnp.transpose(normed, (1, 0, 2)).reshape(block, -1).astype(jnp.bfloat16)
    return lax.map(one_block, query_blocks).reshape(total, -1)

def reference(residual, queries_a, keys_a, values_a, queries_b, keys_b, values_b, mix_lambda, head_gain, out_a, out_b, norm_gain, w_gate, w_up, w_down):
    heads_a = group_attend(queries_a, keys_a, values_a, mix_lambda[0], head_gain[0], QA)
    heads_b = group_attend(queries_b, keys_b, values_b, mix_lambda[1], head_gain[1], QB)
    total = residual.shape[0]
    block = math.gcd(total, 2048)
    count = total // block

    def row_block(inputs):
        residual_rows, first_rows, second_rows = inputs
        mixed = jnp.dot(first_rows, out_a, preferred_element_type=jnp.float32)
        mixed = mixed + jnp.dot(second_rows, out_b, preferred_element_type=jnp.float32)
        summed = residual_rows.astype(jnp.float32) + mixed
        inverse = lax.rsqrt(lax.optimization_barrier(jnp.mean(summed * summed, axis=-1, keepdims=True)) + eps_norm)
        normed = (summed * inverse * norm_gain).astype(jnp.bfloat16)
        gate = jnp.dot(normed, w_gate, preferred_element_type=jnp.float32)
        upward = jnp.dot(normed, w_up, preferred_element_type=jnp.float32)
        hidden = (jax.nn.silu(gate) * upward).astype(jnp.bfloat16)
        channel = jnp.dot(hidden, w_down, preferred_element_type=jnp.float32)
        return (summed + 0.5 * channel).astype(jnp.bfloat16)
    result = lax.map(row_block, (residual.reshape(count, block, -1), heads_a.reshape(count, block, -1), heads_b.reshape(count, block, -1)))
    return result.reshape(total, -1)
```

```python
import functools

import jax
import jax.numpy as jnp
from jax import lax
from jax.experimental import pallas as pl
from jax.experimental.pallas import tpu as pltpu
from jax.sharding import PartitionSpec as P

MESH = pl.DeviceIdType.MESH
F32 = jnp.float32
BF16 = jnp.bfloat16
eps_norm = 1e-06
head_scale = 0.8
log2e = 1.4426950408889634
OFFS = (0, -1, 1, 2)


class Place:
    def __init__(self):
        self.x = lax.axis_index("tp")
        self.me = lax.axis_index("sp")
        self.c = self.me % 2
        y = (self.me // 2) % 4
        z = self.me // 8
        self.z = z
        self.p = y * (1 - self.c) + z * self.c
        self.s = z * (1 - self.c) + y * self.c

    def own(self, dp, ds):
        p, s, c = (self.p + dp + 4) % 4, (self.s + ds + 4) % 4, self.c
        return ((1 - c) * (4 * s + p) + c * (4 * p + s)) * 2 + c

    def other(self, dp, ds):
        p, s, c = (self.s + dp + 4) % 4, (self.p + ds + 4) % 4, 1 - self.c
        return ((1 - c) * (4 * s + p) + c * (4 * p + s)) * 2 + c

    def ring(self, dx):
        return (self.me, (self.x + dx + 4) % 4)


def remote(view, send, recv, device):
    return pltpu.make_async_remote_copy(
        src_ref=view,
        dst_ref=view,
        send_sem=send,
        recv_sem=recv,
        device_id=device,
        device_id_type=MESH,
    )


class Plane:
    count = 36

    def __init__(self, place, whole, half, send, recv):
        self.at, self.whole, self.half, self.send, self.recv = place, whole, half, send, recv

    def copy(self, n):
        at = self.at
        if n < 2:
            view, to = self.whole(at.own(0, 0)), at.own(1 - 2 * n, 0)
        elif n < 4:
            view = self.half(at.own(-1 if n == 2 else 1, 0), n - 2)
            to = at.own(1 if n == 2 else -1, 0)
        elif n < 12:
            view = self.whole(at.own(OFFS[n % 4], 0))
            to = at.own(0, 1 if n < 8 else -1)
        elif n < 20:
            low = n < 16
            view = self.half(at.own(OFFS[n % 4], -1 if low else 1), 0 if low else 1)
            to = at.own(0, 1 if low else -1)
        else:
            view = self.whole(at.own(OFFS[n % 4], (0, -1, 1, 2)[(n - 20) // 4]))
            to = at.other(0, 0)
        return remote(view, self.send.at[n], self.recv.at[n], (to, at.x))

    def go(self, *ns):
        for n in ns:
            self.copy(n).start()

    def come(self, *ns):
        for n in ns:
            self.copy(n).wait_recv()

    def start(self):
        self.go(0, 1, 4, 8, 20)

    def event(self, e):
        line, i = e // 4, e % 4
        if e == 1:
            self.come(0)
            self.go(2, 5, 9)
        elif e == 2:
            self.come(1)
            self.go(3, 6, 10)
        elif e == 3:
            self.come(2, 3)
            self.go(7, 11)
        elif line == 1:
            self.come(4 + i)
            self.go(12 + i)
        elif line == 2:
            self.come(8 + i)
            self.go(16 + i)
        else:
            self.come(12 + i, 16 + i)
        self.go(20 + e)

    def own_block(self, e):
        return self.at.own(OFFS[e % 4], (0, -1, 1, 2)[e // 4])

    def other_block(self, e):
        return self.at.other(OFFS[e % 4], (0, -1, 1, 2)[e // 4])

    def shared(self, e):
        self.come(20 + e)

    def drain(self):
        for n in range(self.count):
            self.copy(n).wait_send()


class Ring:
    def __init__(self, place, whole, half, send, recv, share):
        self.at, self.whole, self.half = place, whole, half
        self.send, self.recv, self.share = send, recv, share

    def copy(self, n):
        at = self.at
        if n < 2:
            view, to = self.whole(at.x), at.ring(1 - 2 * n)
        elif n < 4:
            view = self.half((at.x + (3 if n == 2 else 1)) % 4, n - 2)
            to = at.ring(1 if n == 2 else -1)
        else:
            view, to = self.whole((at.x + (3, 1, 2)[n - 4]) % 4), (at.other(0, 0), at.x)
        return remote(view, self.send.at[n], self.recv.at[n], to)

    def start(self):
        self.copy(0).start()
        self.copy(1).start()

    def relay(self):
        for n in (0, 1):
            self.copy(n).wait_recv()
            self.copy(n + 2).start()
            if self.share:
                self.copy(n + 4).start()

    def last(self):
        self.copy(2).wait_recv()
        self.copy(3).wait_recv()
        if self.share:
            self.copy(6).start()

    def shared(self):
        for n in (4, 5, 6):
            self.copy(n).wait_recv()

    def drain(self):
        for n in range(7 if self.share else 4):
            self.copy(n).wait_send()


RECV = (1, 2, 4, 8, 3, 5, 9, 6, 10, 12, 7, 11, 13, 14, 15)
LAG = 3


def steps():
    order = [("own", 0), ("other", 0)]
    for k in range(len(RECV) + LAG):
        if k < len(RECV):
            order.append(("own", RECV[k]))
        if k >= LAG:
            order.append(("other", RECV[k - LAG]))
    return order


CHUNKS = ((0, 0), (0, 384), (1, 0), (2, 384))


def attend(kv, q_a, q_b, peak, denom, numer, rows):
    key_a = kv[0:rows, 0:128]
    key_1 = kv[0:rows, 128:256]
    key_2 = kv[0:rows, 256:384]
    left = [jnp.concatenate([k, k], 1) for k in (key_a, key_1, key_2)]
    value = [kv[rows : rows + 128, :], kv[rows + 128 : rows + 256, :]]

    def score(chunk):
        which, at = chunk
        q = q_a if which == 0 else q_b
        return jnp.dot(left[which], q[:, at : at + rows], preferred_element_type=F32)

    coming = score(CHUNKS[0])
    for k, (which, at) in enumerate(CHUNKS):
        scores = coming
        if k + 1 < len(CHUNKS):
            coming = score(CHUNKS[k + 1])
        group = min(which, 1)
        cols = slice(at + 2 * rows * group, at + 2 * rows * group + rows)
        before = peak[0:1, cols]
        fresh = jnp.maximum(before, jnp.max(scores, axis=0, keepdims=True))
        decay = jnp.exp2(before - fresh)
        weights = jnp.exp2(scores - fresh)
        peak[0:1, cols] = fresh
        denom[0:1, cols] = denom[0:1, cols] * decay + jnp.sum(weights, axis=0, keepdims=True)
        added = jnp.dot(value[group], weights.astype(BF16), preferred_element_type=F32)
        numer[:, cols] = numer[:, cols] * decay + added


def hi_lo(q, scale):
    wide = jnp.transpose(q.astype(F32) * scale)
    high = wide.astype(BF16).astype(F32)
    return high, wide - high


def kernel(
    residual, queries_a, keys_a, values_a, queries_b, keys_b, values_b, lambdas, head_gain,
    out_a, out_b, norm_gain, w_gate, w_up, w_down, out,
    kv, gu, dn, ow, heads, part, came, res, q_in, v_in, d_in, q_a, q_b, peak, denom, numer,
    summed, normed, gates, hidden, square,
    kv_send, kv_recv, gu_send, gu_recv, dn_send, dn_recv, ow_send, ow_recv,
    hd_send, hd_recv, rs_send, rs_recv, load,
):
    at = Place()
    me, x = at.me, at.x
    rows = residual.shape[0]
    depth = w_gate.shape[0]
    share = out.shape[1]
    inner = w_gate.shape[1]

    def local(n, src, dst):
        return pltpu.make_async_copy(src, dst, load.at[n])

    loads = [
        local(0, keys_a, kv.at[me, 0:rows, 0:128]),
        local(1, keys_b, kv.at[me, 0:rows, 128:384]),
        local(2, values_a, v_in.at[0]),
        local(3, values_b, v_in.at[1]),
        local(4, queries_a, q_in.at[:, 0:128]),
        local(5, queries_b, q_in.at[:, 128:384]),
        local(6, out_a, ow.at[x, 0]),
        local(7, out_b, ow.at[x, 1]),
        local(8, w_gate, gu.at[0, me]),
        local(9, w_up, gu.at[1, me]),
        local(10, w_down, d_in),
        local(11, residual, res),
    ]
    for c in loads:
        c.start()

    barrier = pltpu.get_barrier_semaphore()
    friends = [(at.own(1, 0), x), (at.own(-1, 0), x), (at.own(0, 1), x), (at.own(0, -1), x)]
    friends += [(at.other(0, 0), x), at.ring(1), at.ring(2), at.ring(-1)]
    for f in friends:
        pl.semaphore_signal(barrier, inc=1, device_id=f, device_id_type=MESH)

    for n in (2, 3):
        loads[n].wait()
    for g in range(2):
        kv[me, rows + 128 * g : rows + 128 * (g + 1), :] = jnp.transpose(
            v_in[g].astype(F32)
        ).astype(BF16)
    for n in (0, 1):
        loads[n].wait()
    pl.semaphore_wait(barrier, len(friends))

    cut = (rows + 256) // 2
    KV = Plane(
        at, lambda b: kv.at[b], lambda b, h: kv.at[b, cut * h : cut * (h + 1)], kv_send, kv_recv
    )
    mid = depth // 2
    GU = Plane(
        at,
        lambda b: gu.at[:, b],
        lambda b, h: gu.at[:, b, mid * h : mid * (h + 1)],
        gu_send,
        gu_recv,
    )
    DN = Plane(
        at, lambda b: dn.at[b], lambda b, h: dn.at[b, mid * h : mid * (h + 1)], dn_send, dn_recv
    )
    OW = Ring(
        at,
        lambda b: ow.at[b, at.c],
        lambda b, h: ow.at[b, at.c, 64 * h : 64 * (h + 1)],
        ow_send,
        ow_recv,
        True,
    )
    HD = Ring(
        at,
        lambda b: heads.at[b],
        lambda b, h: heads.at[b, rows // 2 * h : rows // 2 * (h + 1)],
        hd_send,
        hd_recv,
        False,
    )
    KV.start()
    for n in (6, 7):
        loads[n].wait()
    OW.start()

    for n in (4, 5):
        loads[n].wait()
    high, low = hi_lo(q_in[:, 0:128], log2e / 8.0)
    first = lax.broadcasted_iota(jnp.int32, high.shape, 0) < 64
    for j in range(2):
        keep = first if j == 0 else jnp.logical_not(first)
        cols = slice(rows * j, rows * (j + 1))
        q_a[0:128, cols] = jnp.where(keep, high, 0.0).astype(BF16)
        q_a[128:256, cols] = jnp.where(keep, low, 0.0).astype(BF16)
        high_b, low_b = hi_lo(q_in[:, 128 * (j + 1) : 128 * (j + 2)], log2e * 128.0**-0.5)
        q_b[0:128, cols] = high_b.astype(BF16)
        q_b[128:256, cols] = low_b.astype(BF16)
    peak[...] = jnp.full(peak.shape, -1e30, F32)
    denom[...] = jnp.zeros(denom.shape, F32)
    numer[...] = jnp.zeros(numer.shape, F32)
    loads[10].wait()
    dn[me] = jnp.transpose(d_in[...].astype(F32)).astype(BF16)
    for n in (8, 9, 11):
        loads[n].wait()

    order = steps()

    def step(i, carry):
        block = 0
        for k, (whose, e) in enumerate(order):
            b = KV.own_block(e) if whose == "own" else KV.other_block(e)
            block = block + jnp.where(i == k, b, 0)
            if e == 0 and whose == "own":
                continue

            @pl.when(i == k)
            def _(whose=whose, e=e, k=k):
                if whose == "own":
                    KV.event(e)
                    if e == 11:
                        GU.start()
                else:
                    KV.shared(e)
                if k == 10:
                    OW.relay()
                if k == 20:
                    OW.last()

        attend(kv.at[block], q_a, q_b, peak, denom, numer, rows)
        return carry

    lax.fori_loop(0, len(order), step, 0)

    for e in (1, 2, 4, 8):
        GU.event(e)
    ratio = numer[...] / denom[0:1, :]
    for g in range(2):
        base = 2 * rows * g
        mixed = ratio[:, base : base + rows] - lambdas[g, 0] * ratio[:, base + rows : base + 2 * rows]
        scale = lax.rsqrt(jnp.mean(mixed * mixed, axis=0, keepdims=True) + eps_norm)
        done = jnp.transpose(mixed * scale) * head_gain[g : g + 1, :] * head_scale
        heads[x, :, 128 * g : 128 * (g + 1)] = done.astype(BF16)
    HD.start()
    for e in (3, 5, 9):
        GU.event(e)
    HD.relay()
    for e in (6, 10, 12):
        GU.event(e)
    HD.last()
    OW.shared()

    wide = summed.shape[1]
    square[...] = jnp.zeros(square.shape, F32)

    @pl.loop(0, wide // 256)
    def _(n):
        cols = pl.ds(pl.multiple_of(n * 256, 256), 256)
        left = jnp.concatenate([heads[k] for k in range(4)], axis=1)
        right = ow[:, :, :, cols].reshape(1024, 256)
        total = res[:, cols].astype(F32) + jnp.dot(left, right, preferred_element_type=F32)
        summed[:, cols] = total
        twice = total * total
        square[...] += twice[:, 0:128] + twice[:, 128:256]

    inverse = lax.rsqrt(jnp.sum(square[...], axis=1, keepdims=True) / wide + eps_norm)

    @pl.loop(0, wide // 256)
    def _(n):
        cols = pl.ds(pl.multiple_of(n * 256, 256), 256)
        normed[:, cols] = (summed[:, cols] * inverse * norm_gain[0:1, cols]).astype(BF16)

    for e in (7, 11, 13, 14, 15):
        GU.event(e)
        if e == 11:
            DN.start()
    for e in range(16):
        GU.shared(e)

    gates[...] = jnp.zeros(gates.shape, F32)
    pieces = ((0, 512), (512, 512), (1024, inner - 1024))

    @pl.loop(0, 4)
    def _(k):
        left = normed[:, pl.ds(pl.multiple_of(k * 512, 512), 512)]
        for g in range(2):
            for lo, n in pieces:
                right = gu[g, pl.ds(k * 8, 8), :, lo : lo + n].reshape(8 * depth, n)
                gates[g, :, lo : lo + n] += jnp.dot(left, right, preferred_element_type=F32)

    for e in (1, 2, 4, 8, 3, 5, 9, 6, 10, 12):
        DN.event(e)
    for lo, n in pieces:
        gate = gates[0, :, lo : lo + n]
        hidden[:, lo : lo + n] = (gate / (1.0 + jnp.exp(-gate)) * gates[1, :, lo : lo + n]).astype(BF16)
    for e in (7, 11, 13, 14, 15):
        DN.event(e)
    for e in range(16):
        DN.shared(e)

    def give(n):
        return pltpu.make_async_remote_copy(
            src_ref=part.at[(x + n + 1) % 4],
            dst_ref=came.at[n],
            send_sem=rs_send.at[n],
            recv_sem=rs_recv.at[n],
            device_id=at.ring(n + 1),
            device_id_type=MESH,
        )

    for n in (1, 0, 2, 3):
        to = (x + n + 1) % 4
        right = dn[pl.ds(to * 8, 8)].reshape(share, inner)
        sums = lax.dot_general(
            hidden[...], right, (((1,), (1,)), ((), ())), preferred_element_type=F32
        )
        part[to] = sums.astype(BF16)
        if n < 3:
            give(n).start()
    total = part[x].astype(F32)
    for n in range(3):
        give(n).wait_recv()
        total = total + came[n].astype(F32)
    mine = summed[:, pl.ds(pl.multiple_of(x * share, share), share)]
    out[...] = (mine + 0.5 * total).astype(BF16)

    for gather in (KV, GU, DN, OW, HD):
        gather.drain()
    for n in range(3):
        give(n).wait_send()


def local(
    residual, queries_a, keys_a, values_a, queries_b, keys_b, values_b, mix_lambda, head_gain,
    out_a, out_b, norm_gain, w_gate, w_up, w_down,
):
    rows, wide = residual.shape
    depth, inner = w_gate.shape
    share = wide // 4
    anywhere = pl.BlockSpec(memory_space=pl.ANY)
    vmem = pl.BlockSpec(memory_space=pltpu.VMEM)
    smem = pl.BlockSpec(memory_space=pltpu.SMEM)
    dma = pltpu.SemaphoreType.DMA
    count = Plane.count
    return pl.pallas_call(
        kernel,
        out_shape=jax.ShapeDtypeStruct((rows, share), BF16),
        in_specs=[anywhere] * 7 + [smem, vmem, anywhere, anywhere, vmem] + [anywhere] * 3,
        out_specs=vmem,
        scratch_shapes=[
            pltpu.VMEM((32, rows + 256, rows), BF16),
            pltpu.VMEM((2, 32, depth, inner), BF16),
            pltpu.VMEM((32, depth, inner), BF16),
            pltpu.VMEM((4, 2, 128, wide), BF16),
            pltpu.VMEM((4, rows, 256), BF16),
            pltpu.VMEM((4, rows, share), BF16),
            pltpu.VMEM((3, rows, share), BF16),
            pltpu.VMEM((rows, wide), BF16),
            pltpu.VMEM((rows, 384), BF16),
            pltpu.VMEM((2, rows, 128), BF16),
            pltpu.VMEM((inner, depth), BF16),
            pltpu.VMEM((256, 2 * rows), BF16),
            pltpu.VMEM((256, 2 * rows), BF16),
            pltpu.VMEM((1, 4 * rows), F32),
            pltpu.VMEM((1, 4 * rows), F32),
            pltpu.VMEM((128, 4 * rows), F32),
            pltpu.VMEM((rows, wide), F32),
            pltpu.VMEM((rows, wide), BF16),
            pltpu.VMEM((2, rows, inner), F32),
            pltpu.VMEM((rows, inner), BF16),
            pltpu.VMEM((rows, 128), F32),
            dma((count,)), dma((count,)), dma((count,)), dma((count,)), dma((count,)), dma((count,)),
            dma((7,)), dma((7,)), dma((4,)), dma((4,)), dma((3,)), dma((3,)),
            dma((12,)),
        ],
        compiler_params=pltpu.CompilerParams(
            collective_id=0, has_side_effects=True, vmem_limit_bytes=67043328
        ),
        name="layer",
    )(
        residual, queries_a, keys_a, values_a, queries_b, keys_b, values_b, mix_lambda, head_gain,
        out_a, out_b, norm_gain.reshape(1, wide), w_gate, w_up, w_down,
    )


def solution(mesh):
    in_specs = (
        P("sp", None),
        P("sp", "tp"),
        P("sp", "tp"),
        P("sp", "tp"),
        P("sp", "tp"),
        P("sp", "tp"),
        P("sp", "tp"),
        P(None, "tp"),
        P(),
        P("tp", None),
        P("tp", None),
        P(),
        P("sp", "tp"),
        P("sp", "tp"),
        P("tp", "sp"),
    )
    return jax.shard_map(
        local, mesh=mesh, in_specs=in_specs, out_specs=P("sp", "tp"), check_vma=False
    )
```

```python
import functools

import jax
import jax.numpy as jnp
from jax import lax
from jax.experimental import pallas as pl
from jax.experimental.pallas import tpu as pltpu
from jax.sharding import PartitionSpec as P

MESH = pl.DeviceIdType.MESH
F32 = jnp.float32
BF16 = jnp.bfloat16
eps_norm = 1e-06
head_scale = 0.8
log2e = 1.4426950408889634
OFFS = (0, -1, 1, 2)


class Place:
    def __init__(self):
        self.x = lax.axis_index("tp")
        self.me = lax.axis_index("sp")
        self.c = self.me % 2
        y = (self.me // 2) % 4
        z = self.me // 8
        self.z = z
        self.p = y * (1 - self.c) + z * self.c
        self.s = z * (1 - self.c) + y * self.c

    def own(self, dp, ds):
        p, s, c = (self.p + dp + 4) % 4, (self.s + ds + 4) % 4, self.c
        return ((1 - c) * (4 * s + p) + c * (4 * p + s)) * 2 + c

    def other(self, dp, ds):
        p, s, c = (self.s + dp + 4) % 4, (self.p + ds + 4) % 4, 1 - self.c
        return ((1 - c) * (4 * s + p) + c * (4 * p + s)) * 2 + c

    def ring(self, dx):
        return (self.me, (self.x + dx + 4) % 4)


def remote(view, send, recv, device):
    return pltpu.make_async_remote_copy(
        src_ref=view,
        dst_ref=view,
        send_sem=send,
        recv_sem=recv,
        device_id=device,
        device_id_type=MESH,
    )


class Plane:
    count = 36

    def __init__(self, place, whole, half, send, recv):
        self.at, self.whole, self.half, self.send, self.recv = place, whole, half, send, recv

    def copy(self, n):
        at = self.at
        if n < 2:
            view, to = self.whole(at.own(0, 0)), at.own(1 - 2 * n, 0)
        elif n < 4:
            view = self.half(at.own(-1 if n == 2 else 1, 0), n - 2)
            to = at.own(1 if n == 2 else -1, 0)
        elif n < 12:
            view = self.whole(at.own(OFFS[n % 4], 0))
            to = at.own(0, 1 if n < 8 else -1)
        elif n < 20:
            low = n < 16
            view = self.half(at.own(OFFS[n % 4], -1 if low else 1), 0 if low else 1)
            to = at.own(0, 1 if low else -1)
        else:
            view = self.whole(at.own(OFFS[n % 4], (0, -1, 1, 2)[(n - 20) // 4]))
            to = at.other(0, 0)
        return remote(view, self.send.at[n], self.recv.at[n], (to, at.x))

    def go(self, *ns):
        for n in ns:
            self.copy(n).start()

    def come(self, *ns):
        for n in ns:
            self.copy(n).wait_recv()

    def event(self, e):
        line, i = e // 4, e % 4
        if e == 1:
            self.come(0)
            self.go(2, 5, 9)
        elif e == 2:
            self.come(1)
            self.go(3, 6, 10)
        elif e == 3:
            self.come(2, 3)
            self.go(7, 11)
        elif line == 1:
            self.come(4 + i)
            self.go(12 + i)
        elif line == 2:
            self.come(8 + i)
            self.go(16 + i)
        else:
            self.come(12 + i, 16 + i)
        self.go(20 + e)

    def own_block(self, e):
        return self.at.own(OFFS[e % 4], (0, -1, 1, 2)[e // 4])

    def other_block(self, e):
        return self.at.other(OFFS[e % 4], (0, -1, 1, 2)[e // 4])

    def shared(self, e):
        self.come(20 + e)

    def drain(self):
        for n in range(self.count):
            self.copy(n).wait_send()


class Ring:
    def __init__(self, place, whole, half, send, recv, share):
        self.at, self.whole, self.half = place, whole, half
        self.send, self.recv, self.share = send, recv, share

    def copy(self, n):
        at = self.at
        if n < 2:
            view, to = self.whole(at.x), at.ring(1 - 2 * n)
        elif n < 4:
            view = self.half((at.x + (3 if n == 2 else 1)) % 4, n - 2)
            to = at.ring(1 if n == 2 else -1)
        else:
            view, to = self.whole((at.x + (3, 1, 2)[n - 4]) % 4), (at.other(0, 0), at.x)
        return remote(view, self.send.at[n], self.recv.at[n], to)

    def start(self):
        self.copy(0).start()
        self.copy(1).start()

    def relay(self):
        for n in (0, 1):
            self.copy(n).wait_recv()
            self.copy(n + 2).start()
            if self.share:
                self.copy(n + 4).start()

    def last(self):
        self.copy(2).wait_recv()
        self.copy(3).wait_recv()
        if self.share:
            self.copy(6).start()

    def shared(self):
        for n in (4, 5, 6):
            self.copy(n).wait_recv()

    def drain(self):
        for n in range(7 if self.share else 4):
            self.copy(n).wait_send()


RECV = (0, 1, 2, 4, 8, 3, 5, 9, 6, 10, 12, 7, 11, 13, 14, 15)
CHIPS = (
    (0, 0), (0, 1), (0, 2), (1, 0), (2, 0), (1, 1), (1, 2), (2, 1),
    (2, 2), (0, 3), (3, 0), (1, 3), (3, 1), (2, 3), (3, 2), (3, 3),
)


def pick(i, values):
    total = 0
    for k, v in enumerate(values):
        total = total + jnp.where(i == k, v, 0)
    return total


def dispatch(i, jobs, low=0):
    if len(jobs) == 1:
        jobs[0]()
        return
    mid = len(jobs) // 2

    @pl.when(i < low + mid)
    def _():
        dispatch(i, jobs[:mid], low)

    @pl.when(i >= low + mid)
    def _():
        dispatch(i, jobs[mid:], low + mid)


CHUNKS = ((0, 0), (0, 384), (1, 0), (2, 384))


def attend(blocks, q_a, q_b, peak, denom, numer, rows):
    def score(chunk):
        which, at = chunk
        q = q_a if which == 0 else q_b
        found = []
        for kv in blocks:
            key = kv[0:rows, 128 * which : 128 * (which + 1)]
            left = jnp.concatenate([key, key], 1)
            found.append(jnp.dot(left, q[:, at : at + rows], preferred_element_type=F32))
        return found

    coming = score(CHUNKS[0])
    for k, (which, at) in enumerate(CHUNKS):
        scores = coming
        if k + 1 < len(CHUNKS):
            coming = score(CHUNKS[k + 1])
        group = min(which, 1)
        cols = slice(at + 2 * rows * group, at + 2 * rows * group + rows)
        before = peak[0:1, cols]
        fresh = before
        for one in scores:
            fresh = jnp.maximum(fresh, jnp.max(one, axis=0, keepdims=True))
        decay = jnp.exp2(before - fresh)
        weights = [jnp.exp2(one - fresh) for one in scores]
        peak[0:1, cols] = fresh
        total = denom[0:1, cols] * decay
        for one in weights:
            total = total + jnp.sum(one, axis=0, keepdims=True)
        denom[0:1, cols] = total
        value = jnp.concatenate(
            [kv[rows + 128 * group : rows + 128 * (group + 1), :] for kv in blocks], 1
        )
        weights = jnp.concatenate([one.astype(BF16) for one in weights], 0)
        added = jnp.dot(value, weights, preferred_element_type=F32)
        numer[:, cols] = numer[:, cols] * decay + added


def hi_lo(q, scale):
    wide = jnp.transpose(q.astype(F32) * scale)
    high = wide.astype(BF16).astype(F32)
    return high, wide - high


def kernel(
    residual, queries_a, keys_a, values_a, queries_b, keys_b, values_b, lambdas_in, head_gain_in,
    out_a, out_b, norm_gain_in, w_gate, w_up, w_down, out_to,
    lambdas, head_gain, norm_gain, out, kv, gu, dn, ow, heads, part, came, res, q_in, v_in, q_a, q_b, peak, denom, numer,
    summed, normed, gates, hidden, square,
    kv_send, kv_recv, gu_send, gu_recv, dn_recv, ow_send, ow_recv,
    hd_send, hd_recv, rs_send, rs_recv, load, put,
):
    at = Place()
    me, x = at.me, at.x
    rows = residual.shape[0]
    depth = w_gate.shape[0]
    share = out_to.shape[1]
    inner = w_gate.shape[1]

    def local(n, src, dst):
        return pltpu.make_async_copy(src, dst, load.at[n])

    with jax.named_scope("entry"):
        loads = [
            local(0, keys_a, kv.at[me, 0:rows, 0:128]),
            local(1, keys_b, kv.at[me, 0:rows, 128:384]),
            local(2, values_a, v_in.at[0]),
            local(3, values_b, v_in.at[1]),
            local(4, queries_a, q_in.at[:, 0:128]),
            local(5, queries_b, q_in.at[:, 128:384]),
            local(6, out_a, ow.at[x, 0]),
            local(7, out_b, ow.at[x, 1]),
            local(8, w_gate, gu.at[0, me]),
            local(9, w_up, gu.at[1, me]),
            local(10, w_down, dn.at[me]),
            local(11, residual, res),
            local(12, lambdas_in, lambdas),
            local(13, head_gain_in, head_gain),
            local(14, norm_gain_in, norm_gain),
        ]
        for c in loads[:6]:
            c.start()

        barrier = pltpu.get_barrier_semaphore()
        friends = [(at.own(1, 0), x), (at.own(-1, 0), x), (at.own(0, 1), x), (at.own(0, -1), x)]
        friends += [(at.other(0, 0), x), at.ring(1), at.ring(2), at.ring(-1)]
        for f in friends:
            pl.semaphore_signal(barrier, inc=1, device_id=f, device_id_type=MESH)

        for n in (2, 3):
            loads[n].wait()
        for g in range(2):
            kv[me, rows + 128 * g : rows + 128 * (g + 1), :] = jnp.transpose(
                v_in[g].astype(F32)
            ).astype(BF16)
        for n in (0, 1):
            loads[n].wait()
        pl.semaphore_wait(barrier, len(friends))

    cut = (rows + 256) // 2
    KV = Plane(
        at, lambda b: kv.at[b], lambda b, h: kv.at[b, cut * h : cut * (h + 1)], kv_send, kv_recv
    )
    mid = depth // 2
    GU = Plane(
        at,
        lambda b: gu.at[:, b],
        lambda b, h: gu.at[:, b, mid * h : mid * (h + 1)],
        gu_send,
        gu_recv,
    )
    DN = Plane(
        at, lambda b: dn.at[b], lambda b, h: dn.at[b, mid * h : mid * (h + 1)], kv_send, dn_recv
    )
    OW = Ring(
        at,
        lambda b: ow.at[b, at.c],
        lambda b, h: ow.at[b, at.c, 64 * h : 64 * (h + 1)],
        ow_send,
        ow_recv,
        True,
    )
    HD = Ring(
        at,
        lambda b: heads.at[b],
        lambda b, h: heads.at[b, rows // 2 * h : rows // 2 * (h + 1)],
        hd_send,
        hd_recv,
        False,
    )
    with jax.named_scope("prep"):
        KV.go(0, 1, 20)
        for c in loads[6:]:
            c.start()
        for n in (6, 7):
            loads[n].wait()
        OW.start()

        for n in (4, 5):
            loads[n].wait()
        high, low = hi_lo(q_in[:, 0:128], log2e / 8.0)
        first = lax.broadcasted_iota(jnp.int32, high.shape, 0) < 64
        for j in range(2):
            keep = first if j == 0 else jnp.logical_not(first)
            cols = slice(rows * j, rows * (j + 1))
            q_a[0:128, cols] = jnp.where(keep, high, 0.0).astype(BF16)
            q_a[128:256, cols] = jnp.where(keep, low, 0.0).astype(BF16)
            high_b, low_b = hi_lo(q_in[:, 128 * (j + 1) : 128 * (j + 2)], log2e * 128.0**-0.5)
            q_b[0:128, cols] = high_b.astype(BF16)
            q_b[128:256, cols] = low_b.astype(BF16)
        peak[...] = jnp.full(peak.shape, -1e30, F32)
        denom[...] = jnp.zeros(denom.shape, F32)
        numer[...] = jnp.zeros(numer.shape, F32)
        for n in range(8, 15):
            loads[n].wait()

    def take(k):
        def job():
            if k == 1:
                KV.go(4, 8)
                KV.event(RECV[1])
            if 1 <= k < 15:
                KV.event(RECV[k + 1])
            if k == 11:
                GU.go(4, 8, 20)
            if k == 12:
                GU.go(0, 1)
            KV.shared(RECV[k])
            if k == 5:
                OW.relay()
            if k == 10:
                OW.last()

        return job

    turns = [(OFFS[e % 4] + 4) % 4 for e in RECV]
    lines = [(OFFS[e // 4] + 4) % 4 for e in RECV]

    def step(i, carry):
        with jax.named_scope("take"):
            dispatch(i, [take(k) for k in range(16)])
            dp, ds = pick(i, turns), pick(i, lines)
            blocks = [kv.at[at.own(dp, ds)], kv.at[at.other(dp, ds)]]
        with jax.named_scope("attend"):
            attend(blocks, q_a, q_b, peak, denom, numer, rows)
        return carry

    lax.fori_loop(0, 16, step, 0)

    with jax.named_scope("gu_one"):
        GU.event(1)
        GU.event(2)

    with jax.named_scope("finish"):
        ratio = numer[...] / denom[0:1, :]
        for g in range(2):
            base = 2 * rows * g
            mixed = ratio[:, base : base + rows] - lambdas[0, g] * ratio[:, base + rows : base + 2 * rows]
            scale = lax.rsqrt(jnp.mean(mixed * mixed, axis=0, keepdims=True) + eps_norm)
            done = jnp.transpose(mixed * scale) * head_gain[g : g + 1, :] * head_scale
            heads[x, :, 128 * g : 128 * (g + 1)] = done.astype(BF16)
        HD.start()

    with jax.named_scope("gu_two"):
        GU.event(4)
        GU.event(8)
    with jax.named_scope("hd_relay"):
        HD.relay()
    with jax.named_scope("gu_2b"):
        for e in (3, 5, 9):
            GU.event(e)
    with jax.named_scope("hd_last"):
        HD.last()
        OW.shared()
        wide = summed.shape[1]

    with jax.named_scope("project"):
        square[...] = jnp.zeros(square.shape, F32)

        @pl.loop(0, wide // 256)
        def _(n):
            cols = pl.ds(pl.multiple_of(n * 256, 256), 256)
            left = jnp.concatenate([heads[k] for k in range(4)], axis=1)
            right = ow[:, :, :, cols].reshape(1024, 256)
            total = res[:, cols].astype(F32) + jnp.dot(left, right, preferred_element_type=F32)
            summed[:, cols] = total
            twice = total * total
            square[...] += twice[:, 0:128] + twice[:, 128:256]

    with jax.named_scope("gu_three"):
        for e in (6, 10, 12):
            GU.event(e)

    with jax.named_scope("norm"):
        inverse = lax.rsqrt(jnp.sum(square[...], axis=1, keepdims=True) / wide + eps_norm)

        @pl.loop(0, wide // 256)
        def _(n):
            cols = pl.ds(pl.multiple_of(n * 256, 256), 256)
            normed[:, cols] = (summed[:, cols] * inverse * norm_gain[0:1, cols]).astype(BF16)

    pieces = ((0, 512), (512, 512), (1024, inner - 1024))
    with jax.named_scope("gu_four"):
        gates[...] = jnp.zeros(gates.shape, F32)
        KV.drain()
        OW.drain()
        HD.drain()

    def line(k):
        def job():
            if k == 1:
                GU.event(7)
                GU.event(11)
                DN.go(4, 8, 20, 0, 1)
            if k > 0:
                GU.event(12 + k)
            if k == 3:
                DN.event(1)
                DN.event(2)
            for other in range(4):
                GU.shared(4 * other + k)

        return job

    def gate_step(k, carry):
        with jax.named_scope("line"):
            dispatch(k, [line(n) for n in range(4)])
            s = (at.s + pick(k, (0, 3, 1, 2))) % 4
            chips = [(1 - at.c) * (4 * s + n) + at.c * (4 * n + s) for n in range(4)]
        with jax.named_scope("gate"):
            left = jnp.concatenate(
                [normed[:, pl.ds(pl.multiple_of(n * 128, 128), 128)] for n in chips], axis=1
            )
            for g in range(2):
                for lo, n in pieces:
                    right = jnp.concatenate(
                        [gu[g, pl.ds(2 * m, 2), :, lo : lo + n].reshape(128, n) for m in chips],
                        axis=0,
                    )
                    gates[g, :, lo : lo + n] += jnp.dot(left, right, preferred_element_type=F32)
        return carry

    lax.fori_loop(0, 4, gate_step, 0)

    with jax.named_scope("act"):
        for lo, n in pieces:
            gate = gates[0, :, lo : lo + n]
            hidden[:, lo : lo + n] = (
                gate / (1.0 + jnp.exp(-gate)) * gates[1, :, lo : lo + n]
            ).astype(BF16)

    with jax.named_scope("dn_one"):
        DN.event(4)
        DN.event(8)
        GU.drain()

    def give(chip):
        to, y = chip // 4, chip % 4
        slot = (to - x + 3) % 4
        return pltpu.make_async_remote_copy(
            src_ref=part.at[chip],
            dst_ref=came.at[slot, y],
            send_sem=rs_send.at[chip],
            recv_sem=rs_recv.at[4 * slot + y],
            device_id=(me, to),
            device_id_type=MESH,
        )

    down_events = ((), (), (3, 5, 9), (6, 10), (12,), (7, 11, 13), (14,), (15,))
    down_shared = ((0, 1), (2, 4), (8, 5), (6, 9), (10, 3), (12, 7), (13, 11), (14, 15))

    def arrive(k):
        def job():
            for e in down_events[k]:
                DN.event(e)
            for e in down_shared[k]:
                DN.shared(e)

        return job

    offsets = (0, 3, 1, 2)

    def down_step(k, carry):
        with jax.named_scope("arrive"):
            dispatch(k, [arrive(n) for n in range(8)])
            chips = []
            for n in range(2):
                dp = pick(k, [offsets[a] for a, _ in CHIPS[n::2]])
                ds = pick(k, [offsets[b] for _, b in CHIPS[n::2]])
                chips.append(at.own(dp, ds) // 2)
        with jax.named_scope("down"):
            right = jnp.concatenate(
                [dn[pl.ds(2 * m, 2)].reshape(128, inner) for m in chips], axis=0
            )
            sums = lax.dot_general(
                hidden[...], right, (((1,), (1,)), ((), ())), preferred_element_type=F32
            ).astype(BF16)
            for n, m in enumerate(chips):
                part[m] = sums[:, 128 * n : 128 * (n + 1)]
        with jax.named_scope("give"):
            for m in chips:

                @pl.when(m // 4 != x)
                def _(m=m):
                    give(m).start()
        return carry

    lax.fori_loop(0, 8, down_step, 0)

    with jax.named_scope("sum"):
        for y in range(4):
            total = part[4 * x + y].astype(F32)
            for slot in range(3):
                pltpu.make_async_remote_copy(
                    src_ref=part.at[y],
                    dst_ref=came.at[slot, y],
                    send_sem=rs_send.at[y],
                    recv_sem=rs_recv.at[4 * slot + y],
                    device_id=at.ring(1),
                    device_id_type=MESH,
                ).wait_recv()
                total = total + came[slot, y].astype(F32)
            cols = pl.ds(pl.multiple_of(x * share + 128 * y, 128), 128)
            out[:, 128 * y : 128 * (y + 1)] = (summed[:, cols] + 0.5 * total).astype(BF16)
        done = pltpu.make_async_copy(out, out_to, put)
        done.start()

    with jax.named_scope("drain"):
        DN.drain()
        for n in range(1, 4):
            for y in range(4):
                give(4 * ((x + n) % 4) + y).wait_send()
        done.wait()


def local(
    residual, queries_a, keys_a, values_a, queries_b, keys_b, values_b, mix_lambda, head_gain,
    out_a, out_b, norm_gain, w_gate, w_up, w_down,
):
    rows, wide = residual.shape
    depth, inner = w_gate.shape
    share = wide // 4
    anywhere = pl.BlockSpec(memory_space=pl.ANY)
    dma = pltpu.SemaphoreType.DMA
    count = Plane.count
    return pl.pallas_call(
        kernel,
        out_shape=jax.ShapeDtypeStruct((rows, share), BF16),
        in_specs=[anywhere] * 15,
        out_specs=anywhere,
        scratch_shapes=[
            pltpu.SMEM((1, 2), F32),
            pltpu.VMEM((2, 128), F32),
            pltpu.VMEM((1, wide), F32),
            pltpu.VMEM((rows, share), BF16),
            pltpu.VMEM((32, rows + 256, rows), BF16),
            pltpu.VMEM((2, 32, depth, inner), BF16),
            pltpu.VMEM((32, depth, inner), BF16),
            pltpu.VMEM((4, 2, 128, wide), BF16),
            pltpu.VMEM((4, rows, 256), BF16),
            pltpu.VMEM((16, rows, 128), BF16),
            pltpu.VMEM((3, 4, rows, 128), BF16),
            pltpu.VMEM((rows, wide), BF16),
            pltpu.VMEM((rows, 384), BF16),
            pltpu.VMEM((2, rows, 128), BF16),
            pltpu.VMEM((256, 2 * rows), BF16),
            pltpu.VMEM((256, 2 * rows), BF16),
            pltpu.VMEM((1, 4 * rows), F32),
            pltpu.VMEM((1, 4 * rows), F32),
            pltpu.VMEM((128, 4 * rows), F32),
            pltpu.VMEM((rows, wide), F32),
            pltpu.VMEM((rows, wide), BF16),
            pltpu.VMEM((2, rows, inner), F32),
            pltpu.VMEM((rows, inner), BF16),
            pltpu.VMEM((rows, 128), F32),
            dma((count,)), dma((count,)), dma((count,)), dma((count,)), dma((count,)),
            dma((7,)), dma((7,)), dma((4,)), dma((4,)), dma((16,)), dma((12,)),
            dma((15,)), dma,
        ],
        compiler_params=pltpu.CompilerParams(
            collective_id=0, has_side_effects=True, vmem_limit_bytes=67043328
        ),
        name="layer",
    )(
        residual, queries_a, keys_a, values_a, queries_b, keys_b, values_b, mix_lambda.T, head_gain,
        out_a, out_b, norm_gain.reshape(1, wide), w_gate, w_up, w_down.T,
    )


def solution(mesh):
    in_specs = (
        P("sp", None),
        P("sp", "tp"),
        P("sp", "tp"),
        P("sp", "tp"),
        P("sp", "tp"),
        P("sp", "tp"),
        P("sp", "tp"),
        P(None, "tp"),
        P(),
        P("tp", None),
        P("tp", None),
        P(),
        P("sp", "tp"),
        P("sp", "tp"),
        P("tp", "sp"),
    )
    return jax.shard_map(
        local, mesh=mesh, in_specs=in_specs, out_specs=P("sp", "tp"), check_vma=False
    )
```

```python
import functools

import jax
import jax.numpy as jnp
from jax import lax
from jax.experimental import pallas as pl
from jax.experimental.pallas import tpu as pltpu
from jax.sharding import PartitionSpec as P

MESH = pl.DeviceIdType.MESH
F32 = jnp.float32
BF16 = jnp.bfloat16
eps_norm = 1e-06
head_scale = 0.8
log2e = 1.4426950408889634
OFFS = (0, -1, 1, 2)


class Place:
    def __init__(self):
        self.x = lax.axis_index("tp")
        self.me = lax.axis_index("sp")
        self.c = self.me % 2
        y = (self.me // 2) % 4
        z = self.me // 8
        self.z = z
        self.p = y * (1 - self.c) + z * self.c
        self.s = z * (1 - self.c) + y * self.c

    def own(self, dp, ds):
        p, s, c = (self.p + dp + 4) % 4, (self.s + ds + 4) % 4, self.c
        return ((1 - c) * (4 * s + p) + c * (4 * p + s)) * 2 + c

    def other(self, dp, ds):
        p, s, c = (self.s + dp + 4) % 4, (self.p + ds + 4) % 4, 1 - self.c
        return ((1 - c) * (4 * s + p) + c * (4 * p + s)) * 2 + c

    def ring(self, dx):
        return (self.me, (self.x + dx + 4) % 4)


def remote(view, send, recv, device):
    return pltpu.make_async_remote_copy(
        src_ref=view,
        dst_ref=view,
        send_sem=send,
        recv_sem=recv,
        device_id=device,
        device_id_type=MESH,
    )


class Plane:
    count = 36

    def __init__(self, place, whole, half, send, recv):
        self.at, self.whole, self.half, self.send, self.recv = place, whole, half, send, recv

    def copy(self, n):
        at = self.at
        if n < 2:
            view, to = self.whole(at.own(0, 0)), at.own(1 - 2 * n, 0)
        elif n < 4:
            view = self.half(at.own(-1 if n == 2 else 1, 0), n - 2)
            to = at.own(1 if n == 2 else -1, 0)
        elif n < 12:
            view = self.whole(at.own(OFFS[n % 4], 0))
            to = at.own(0, 1 if n < 8 else -1)
        elif n < 20:
            low = n < 16
            view = self.half(at.own(OFFS[n % 4], -1 if low else 1), 0 if low else 1)
            to = at.own(0, 1 if low else -1)
        else:
            view = self.whole(at.own(OFFS[n % 4], (0, -1, 1, 2)[(n - 20) // 4]))
            to = at.other(0, 0)
        return remote(view, self.send.at[n], self.recv.at[n], (to, at.x))

    def go(self, *ns):
        for n in ns:
            self.copy(n).start()

    def come(self, *ns):
        for n in ns:
            self.copy(n).wait_recv()

    def event(self, e):
        line, i = e // 4, e % 4
        if e == 1:
            self.come(0)
            self.go(2, 5, 9)
        elif e == 2:
            self.come(1)
            self.go(3, 6, 10)
        elif e == 3:
            self.come(2, 3)
            self.go(7, 11)
        elif line == 1:
            self.come(4 + i)
            self.go(12 + i)
        elif line == 2:
            self.come(8 + i)
            self.go(16 + i)
        else:
            self.come(12 + i, 16 + i)
        self.go(20 + e)

    def own_block(self, e):
        return self.at.own(OFFS[e % 4], (0, -1, 1, 2)[e // 4])

    def other_block(self, e):
        return self.at.other(OFFS[e % 4], (0, -1, 1, 2)[e // 4])

    def shared(self, e):
        self.come(20 + e)

    def drain(self):
        for n in range(self.count):
            self.copy(n).wait_send()


class Ring:
    def __init__(self, place, whole, half, send, recv, share):
        self.at, self.whole, self.half = place, whole, half
        self.send, self.recv, self.share = send, recv, share

    def copy(self, n):
        at = self.at
        if n < 2:
            view, to = self.whole(at.x), at.ring(1 - 2 * n)
        elif n < 4:
            view = self.half((at.x + (3 if n == 2 else 1)) % 4, n - 2)
            to = at.ring(1 if n == 2 else -1)
        else:
            view, to = self.whole((at.x + (3, 1, 2)[n - 4]) % 4), (at.other(0, 0), at.x)
        return remote(view, self.send.at[n], self.recv.at[n], to)

    def start(self):
        self.copy(0).start()
        self.copy(1).start()

    def relay(self):
        for n in (0, 1):
            self.copy(n).wait_recv()
            self.copy(n + 2).start()
            if self.share:
                self.copy(n + 4).start()

    def last(self):
        self.copy(2).wait_recv()
        self.copy(3).wait_recv()
        if self.share:
            self.copy(6).start()

    def shared(self):
        for n in (4, 5, 6):
            self.copy(n).wait_recv()

    def drain(self):
        for n in range(7 if self.share else 4):
            self.copy(n).wait_send()


RECV = (0, 1, 2, 4, 8, 3, 5, 9, 6, 10, 12, 7, 11, 13, 14, 15)
CHIPS = (
    (0, 0), (0, 1), (0, 2), (1, 0), (2, 0), (1, 1), (1, 2), (2, 1),
    (2, 2), (0, 3), (3, 0), (1, 3), (3, 1), (2, 3), (3, 2), (3, 3),
)


LAG = 3


def pick(i, values):
    total = 0
    for k, v in enumerate(values):
        total = total + jnp.where(i == k, v, 0)
    return total


def dispatch(i, jobs, low=0):
    if len(jobs) == 1:
        jobs[0]()
        return
    mid = len(jobs) // 2

    @pl.when(i < low + mid)
    def _():
        dispatch(i, jobs[:mid], low)

    @pl.when(i >= low + mid)
    def _():
        dispatch(i, jobs[mid:], low + mid)


CHUNKS = ((0, 0), (0, 384), (1, 0), (2, 384))


def attend(blocks, q_a, q_b, peak, denom, numer, rows):
    def score(chunk):
        which, at = chunk
        q = q_a if which == 0 else q_b
        found = []
        for kv in blocks:
            key = kv[0:rows, 128 * which : 128 * (which + 1)]
            left = jnp.concatenate([key, key], 1)
            found.append(jnp.dot(left, q[:, at : at + rows], preferred_element_type=F32))
        return found

    coming = score(CHUNKS[0])
    for k, (which, at) in enumerate(CHUNKS):
        scores = coming
        if k + 1 < len(CHUNKS):
            coming = score(CHUNKS[k + 1])
        group = min(which, 1)
        cols = slice(at + 2 * rows * group, at + 2 * rows * group + rows)
        before = peak[0:1, cols]
        fresh = before
        for one in scores:
            fresh = jnp.maximum(fresh, jnp.max(one, axis=0, keepdims=True))
        decay = jnp.exp2(before - fresh)
        weights = [jnp.exp2(one - fresh) for one in scores]
        peak[0:1, cols] = fresh
        total = denom[0:1, cols] * decay
        for one in weights:
            total = total + jnp.sum(one, axis=0, keepdims=True)
        denom[0:1, cols] = total
        value = jnp.concatenate(
            [kv[rows + 128 * group : rows + 128 * (group + 1), :] for kv in blocks], 1
        )
        weights = jnp.concatenate([one.astype(BF16) for one in weights], 0)
        added = jnp.dot(value, weights, preferred_element_type=F32)
        numer[:, cols] = numer[:, cols] * decay + added


def hi_lo(q, scale):
    wide = jnp.transpose(q.astype(F32) * scale)
    high = wide.astype(BF16).astype(F32)
    return high, wide - high


def kernel(
    residual, queries_a, keys_a, values_a, queries_b, keys_b, values_b, lambdas_in, head_gain_in,
    out_a, out_b, norm_gain_in, w_gate, w_up, w_down, out,
    lambdas, head_gain, norm_gain, kv, gu, dn, ow, heads, part, came, passing, res, q_in, v_in, q_a, q_b, peak, denom, numer,
    summed, normed, gates, hidden, square,
    kv_send, kv_recv, gu_send, gu_recv, dn_recv, ow_send, ow_recv,
    hd_send, hd_recv, rs_send, rs_recv, ps_recv, load,
):
    at = Place()
    me, x = at.me, at.x
    rows = residual.shape[0]
    depth = w_gate.shape[0]
    share = out.shape[1]
    inner = w_gate.shape[1]

    def local(n, src, dst):
        return pltpu.make_async_copy(src, dst, load.at[n])

    with jax.named_scope("entry"):
        loads = [
            local(0, keys_a, kv.at[me, 0:rows, 0:128]),
            local(1, keys_b, kv.at[me, 0:rows, 128:384]),
            local(2, values_a, v_in.at[0]),
            local(3, values_b, v_in.at[1]),
            local(4, queries_a, q_in.at[:, 0:128]),
            local(5, queries_b, q_in.at[:, 128:384]),
            local(6, out_a, ow.at[x, 0]),
            local(7, out_b, ow.at[x, 1]),
            local(8, w_gate, gu.at[0, me]),
            local(9, w_up, gu.at[1, me]),
            local(10, w_down, dn.at[me]),
            local(11, residual, res),
            local(12, lambdas_in, lambdas),
            local(13, head_gain_in, head_gain),
            local(14, norm_gain_in, norm_gain),
        ]
        for c in loads[:6]:
            c.start()

        barrier = pltpu.get_barrier_semaphore()
        friends = [(at.own(1, 0), x), (at.own(-1, 0), x), (at.own(0, 1), x), (at.own(0, -1), x)]
        friends += [(at.other(0, 0), x), at.ring(1), at.ring(2), at.ring(-1)]
        for f in friends:
            pl.semaphore_signal(barrier, inc=1, device_id=f, device_id_type=MESH)

        for n in (2, 3):
            loads[n].wait()
        for g in range(2):
            kv[me, rows + 128 * g : rows + 128 * (g + 1), :] = jnp.transpose(
                v_in[g].astype(F32)
            ).astype(BF16)
        for n in (0, 1):
            loads[n].wait()
        pl.semaphore_wait(barrier, len(friends))

    cut = (rows + 256) // 2
    KV = Plane(
        at, lambda b: kv.at[b], lambda b, h: kv.at[b, cut * h : cut * (h + 1)], kv_send, kv_recv
    )
    mid = depth // 2
    GU = Plane(
        at,
        lambda b: gu.at[:, b],
        lambda b, h: gu.at[:, b, mid * h : mid * (h + 1)],
        gu_send,
        gu_recv,
    )
    DN = Plane(
        at, lambda b: dn.at[b], lambda b, h: dn.at[b, mid * h : mid * (h + 1)], kv_send, dn_recv
    )
    OW = Ring(
        at,
        lambda b: ow.at[b, at.c],
        lambda b, h: ow.at[b, at.c, 64 * h : 64 * (h + 1)],
        ow_send,
        ow_recv,
        True,
    )
    HD = Ring(
        at,
        lambda b: heads.at[b],
        lambda b, h: heads.at[b, rows // 2 * h : rows // 2 * (h + 1)],
        hd_send,
        hd_recv,
        False,
    )
    with jax.named_scope("prep"):
        KV.go(0, 1, 4, 8, 20)
        for c in loads[6:]:
            c.start()
        for n in (6, 7):
            loads[n].wait()
        OW.start()

        for n in (4, 5):
            loads[n].wait()
        high, low = hi_lo(q_in[:, 0:128], log2e / 8.0)
        first = lax.broadcasted_iota(jnp.int32, high.shape, 0) < 64
        for j in range(2):
            keep = first if j == 0 else jnp.logical_not(first)
            cols = slice(rows * j, rows * (j + 1))
            q_a[0:128, cols] = jnp.where(keep, high, 0.0).astype(BF16)
            q_a[128:256, cols] = jnp.where(keep, low, 0.0).astype(BF16)
            high_b, low_b = hi_lo(q_in[:, 128 * (j + 1) : 128 * (j + 2)], log2e * 128.0**-0.5)
            q_b[0:128, cols] = high_b.astype(BF16)
            q_b[128:256, cols] = low_b.astype(BF16)
        peak[...] = jnp.full(peak.shape, -1e30, F32)
        denom[...] = jnp.zeros(denom.shape, F32)
        numer[...] = jnp.zeros(numer.shape, F32)
        for n in range(8, 15):
            loads[n].wait()

    def take(k):
        def job():
            if k == 1:
                KV.event(RECV[1])
            if 1 <= k < 15:
                KV.event(RECV[k + 1])
            if k == 11:
                GU.go(4, 8, 20)
            if k == 12:
                GU.go(0, 1)
            KV.shared(RECV[k])
            if k == 5:
                OW.relay()
            if k == 10:
                OW.last()

        return job

    turns = [(OFFS[e % 4] + 4) % 4 for e in RECV]
    lines = [(OFFS[e // 4] + 4) % 4 for e in RECV]

    def step(i, carry):
        with jax.named_scope("take"):
            dispatch(i, [take(k) for k in range(16)])
            dp, ds = pick(i, turns), pick(i, lines)
            blocks = [kv.at[at.own(dp, ds)], kv.at[at.other(dp, ds)]]
        with jax.named_scope("attend"):
            attend(blocks, q_a, q_b, peak, denom, numer, rows)
        return carry

    lax.fori_loop(0, 16, step, 0)

    with jax.named_scope("gu_one"):
        GU.event(1)
        GU.event(2)

    with jax.named_scope("finish"):
        ratio = numer[...] / denom[0:1, :]
        for g in range(2):
            base = 2 * rows * g
            mixed = ratio[:, base : base + rows] - lambdas[0, g] * ratio[:, base + rows : base + 2 * rows]
            scale = lax.rsqrt(jnp.mean(mixed * mixed, axis=0, keepdims=True) + eps_norm)
            done = jnp.transpose(mixed * scale) * head_gain[g : g + 1, :] * head_scale
            heads[x, :, 128 * g : 128 * (g + 1)] = done.astype(BF16)
        HD.start()

    with jax.named_scope("gu_two"):
        GU.event(4)
        GU.event(8)
    with jax.named_scope("hd_relay"):
        HD.relay()
    with jax.named_scope("gu_2b"):
        for e in (3, 5, 9):
            GU.event(e)
    with jax.named_scope("hd_last"):
        HD.last()
        OW.shared()
        wide = summed.shape[1]

    with jax.named_scope("project"):
        square[...] = jnp.zeros(square.shape, F32)

        @pl.loop(0, wide // 256)
        def _(n):
            cols = pl.ds(pl.multiple_of(n * 256, 256), 256)
            left = jnp.concatenate([heads[k] for k in range(4)], axis=1)
            right = ow[:, :, :, cols].reshape(1024, 256)
            total = res[:, cols].astype(F32) + jnp.dot(left, right, preferred_element_type=F32)
            summed[:, cols] = total
            twice = total * total
            square[...] += twice[:, 0:128] + twice[:, 128:256]

    with jax.named_scope("gu_three"):
        for e in (6, 10, 12):
            GU.event(e)

    with jax.named_scope("norm"):
        inverse = lax.rsqrt(jnp.sum(square[...], axis=1, keepdims=True) / wide + eps_norm)

        @pl.loop(0, wide // 256)
        def _(n):
            cols = pl.ds(pl.multiple_of(n * 256, 256), 256)
            normed[:, cols] = (summed[:, cols] * inverse * norm_gain[0:1, cols]).astype(BF16)

    pieces = ((0, 512), (512, 512), (1024, inner - 1024))
    with jax.named_scope("gu_four"):
        gates[...] = jnp.zeros(gates.shape, F32)
        KV.drain()
        OW.drain()
        HD.drain()

    def line(k):
        def job():
            if k == 1:
                GU.event(7)
                GU.event(11)
                DN.go(4, 8, 20, 0, 1)
            if k > 0:
                GU.event(12 + k)
            if k == 3:
                DN.event(1)
                DN.event(2)
            for other in range(4):
                GU.shared(4 * other + k)

        return job

    def gate_step(k, carry):
        with jax.named_scope("line"):
            dispatch(k, [line(n) for n in range(4)])
            s = (at.s + pick(k, (0, 3, 1, 2))) % 4
            chips = [(1 - at.c) * (4 * s + n) + at.c * (4 * n + s) for n in range(4)]
        with jax.named_scope("gate"):
            left = jnp.concatenate(
                [normed[:, pl.ds(pl.multiple_of(n * 128, 128), 128)] for n in chips], axis=1
            )
            for g in range(2):
                for lo, n in pieces:
                    right = jnp.concatenate(
                        [gu[g, pl.ds(2 * m, 2), :, lo : lo + n].reshape(128, n) for m in chips],
                        axis=0,
                    )
                    gates[g, :, lo : lo + n] += jnp.dot(left, right, preferred_element_type=F32)
        return carry

    lax.fori_loop(0, 4, gate_step, 0)

    with jax.named_scope("act"):
        for lo, n in pieces:
            gate = gates[0, :, lo : lo + n]
            hidden[:, lo : lo + n] = (
                gate / (1.0 + jnp.exp(-gate)) * gates[1, :, lo : lo + n]
            ).astype(BF16)

    with jax.named_scope("dn_one"):
        DN.event(4)
        DN.event(8)
        GU.drain()

    half = rows // 2

    def give(chip, h, to, target, arrived, n):
        return pltpu.make_async_remote_copy(
            src_ref=part.at[chip, half * h : half * (h + 1)],
            dst_ref=target,
            send_sem=rs_send.at[2 * chip + n],
            recv_sem=arrived,
            device_id=(me, to),
            device_id_type=MESH,
        )

    def side(chip, n, h):
        y = chip % 4
        target = came.at[n, y, half * h : half * (h + 1)]
        return give(chip, h, chip // 4, target, rs_recv.at[8 * n + 2 * y + h], h)

    def through(chip, n):
        y = chip % 4
        return give(chip, n, (x + 1 + 2 * n) % 4, passing.at[n, y], ps_recv.at[4 * n + y], n)

    def first_give(chip):
        away = (chip // 4 - x + 4) % 4

        @pl.when(away == 2)
        def _():
            through(chip, 0).start()
            through(chip, 1).start()

        for n in range(2):

            @pl.when(away == 1 + 2 * n)
            def _(n=n):
                side(chip, n, 1 - n).start()

    def second_give(chip):
        y = chip % 4
        away = (chip // 4 - x + 4) % 4
        for n in range(2):

            @pl.when(away == 1 + 2 * n)
            def _(n=n):
                through(chip, n).wait_recv()
                mine = part[chip, half * n : half * (n + 1)].astype(F32)
                mine = mine + passing[n, y].astype(F32)
                part[chip, half * n : half * (n + 1)] = mine.astype(BF16)
                side(chip, n, n).start()

    down_events = ((), (), (3, 5, 9), (6, 10), (12,), (7, 11, 13), (14,), (15,))
    down_shared = ((0, 1), (2, 4), (8, 5), (6, 9), (10, 3), (12, 7), (13, 11), (14, 15))

    def arrive(k):
        def job():
            for e in down_events[k]:
                DN.event(e)
            for e in down_shared[k]:
                DN.shared(e)

        return job

    offsets = (0, 3, 1, 2)

    def chips_of(k):
        found = []
        for n in range(2):
            dp = pick(k, [offsets[a] for a, _ in CHIPS[n::2]])
            ds = pick(k, [offsets[b] for _, b in CHIPS[n::2]])
            found.append(at.own(dp, ds) // 2)
        return found

    def down_step(k, carry):
        with jax.named_scope("arrive"):
            dispatch(k, [arrive(n) for n in range(8)])
            chips = chips_of(k)
        with jax.named_scope("down"):
            right = jnp.concatenate(
                [dn[pl.ds(2 * m, 2)].reshape(128, inner) for m in chips], axis=0
            )
            sums = lax.dot_general(
                hidden[...], right, (((1,), (1,)), ((), ())), preferred_element_type=F32
            ).astype(BF16)
            for n, m in enumerate(chips):
                part[m] = sums[:, 128 * n : 128 * (n + 1)]
        with jax.named_scope("give"):
            for m in chips:
                first_give(m)

        with jax.named_scope("second"):

            @pl.when(k >= LAG)
            def _():
                for m in chips_of(k - LAG):
                    second_give(m)

        return carry

    lax.fori_loop(0, 8, down_step, 0)

    with jax.named_scope("late"):

        @pl.loop(8 - LAG, 8)
        def _(k):
            for m in chips_of(k):
                second_give(m)

    with jax.named_scope("sum"):

        def sum_step(k, carry):
            for m in chips_of(k):

                @pl.when(m // 4 == x)
                def _(m=m):
                    y = m % 4
                    cols = pl.ds(pl.multiple_of(x * share + 128 * y, 128), 128)
                    into = pl.ds(pl.multiple_of(128 * y, 128), 128)
                    for n in range(2):
                        for h in range(2):
                            side(m, n, h).wait_recv()
                    total = (
                        part[m].astype(F32) + came[0, y].astype(F32) + came[1, y].astype(F32)
                    )
                    out[:, into] = (summed[:, cols] + 0.5 * total).astype(BF16)

            return carry

        lax.fori_loop(0, 8, sum_step, 0)

    with jax.named_scope("drain"):
        DN.drain()
        for n in range(1, 4):
            for y in range(4):
                for h in range(2):
                    side(4 * ((x + n) % 4) + y, 0, h).wait_send()


def local(
    residual, queries_a, keys_a, values_a, queries_b, keys_b, values_b, mix_lambda, head_gain,
    out_a, out_b, norm_gain, w_gate, w_up, w_down,
):
    rows, wide = residual.shape
    depth, inner = w_gate.shape
    share = wide // 4
    anywhere = pl.BlockSpec(memory_space=pl.ANY)
    dma = pltpu.SemaphoreType.DMA
    count = Plane.count
    return pl.pallas_call(
        kernel,
        out_shape=pltpu.VMEM((rows, share), BF16),
        in_specs=[anywhere] * 15,
        out_specs=pl.BlockSpec(memory_space=pltpu.VMEM),
        scratch_shapes=[
            pltpu.SMEM((1, 2), F32),
            pltpu.VMEM((2, 128), F32),
            pltpu.VMEM((1, wide), F32),
            pltpu.VMEM((32, rows + 256, rows), BF16),
            pltpu.VMEM((2, 32, depth, inner), BF16),
            pltpu.VMEM((32, depth, inner), BF16),
            pltpu.VMEM((4, 2, 128, wide), BF16),
            pltpu.VMEM((4, rows, 256), BF16),
            pltpu.VMEM((16, rows, 128), BF16),
            pltpu.VMEM((2, 4, rows, 128), BF16),
            pltpu.VMEM((2, 4, rows // 2, 128), BF16),
            pltpu.VMEM((rows, wide), BF16),
            pltpu.VMEM((rows, 384), BF16),
            pltpu.VMEM((2, rows, 128), BF16),
            pltpu.VMEM((256, 2 * rows), BF16),
            pltpu.VMEM((256, 2 * rows), BF16),
            pltpu.VMEM((1, 4 * rows), F32),
            pltpu.VMEM((1, 4 * rows), F32),
            pltpu.VMEM((128, 4 * rows), F32),
            pltpu.VMEM((rows, wide), F32),
            pltpu.VMEM((rows, wide), BF16),
            pltpu.VMEM((2, rows, inner), F32),
            pltpu.VMEM((rows, inner), BF16),
            pltpu.VMEM((rows, 128), F32),
            dma((count,)), dma((count,)), dma((count,)), dma((count,)), dma((count,)),
            dma((7,)), dma((7,)), dma((4,)), dma((4,)), dma((32,)), dma((16,)), dma((8,)),
            dma((15,)),
        ],
        compiler_params=pltpu.CompilerParams(
            collective_id=0, has_side_effects=True, vmem_limit_bytes=66 * 1000 * 1000
        ),
        name="layer",
    )(
        residual, queries_a, keys_a, values_a, queries_b, keys_b, values_b, mix_lambda.T, head_gain,
        out_a, out_b, norm_gain.reshape(1, wide), w_gate, w_up, w_down.T,
    )


def solution(mesh):
    in_specs = (
        P("sp", None),
        P("sp", "tp"),
        P("sp", "tp"),
        P("sp", "tp"),
        P("sp", "tp"),
        P("sp", "tp"),
        P("sp", "tp"),
        P(None, "tp"),
        P(),
        P("tp", None),
        P("tp", None),
        P(),
        P("sp", "tp"),
        P("sp", "tp"),
        P("tp", "sp"),
    )
    return jax.shard_map(
        local, mesh=mesh, in_specs=in_specs, out_specs=P("sp", "tp"), check_vma=False
    )
```

```python
import functools

import jax
import jax.numpy as jnp
from jax import lax
from jax.experimental import pallas as pl
from jax.experimental.pallas import tpu as pltpu
from jax.sharding import PartitionSpec as P

MESH = pl.DeviceIdType.MESH
F32 = jnp.float32
BF16 = jnp.bfloat16
eps_norm = 1e-06
head_scale = 0.8
log2e = 1.4426950408889634
OFFS = (0, -1, 1, 2)


class Place:
    def __init__(self):
        self.x = lax.axis_index("tp")
        self.me = lax.axis_index("sp")
        self.c = self.me % 2
        y = (self.me // 2) % 4
        z = self.me // 8
        self.z = z
        self.p = y * (1 - self.c) + z * self.c
        self.s = z * (1 - self.c) + y * self.c

    def own(self, dp, ds):
        p, s, c = (self.p + dp + 4) % 4, (self.s + ds + 4) % 4, self.c
        return ((1 - c) * (4 * s + p) + c * (4 * p + s)) * 2 + c

    def other(self, dp, ds):
        p, s, c = (self.s + dp + 4) % 4, (self.p + ds + 4) % 4, 1 - self.c
        return ((1 - c) * (4 * s + p) + c * (4 * p + s)) * 2 + c

    def ring(self, dx):
        return (self.me, (self.x + dx + 4) % 4)


def remote(view, send, recv, device):
    return pltpu.make_async_remote_copy(
        src_ref=view,
        dst_ref=view,
        send_sem=send,
        recv_sem=recv,
        device_id=device,
        device_id_type=MESH,
    )


class Plane:
    count = 36

    def __init__(self, place, whole, half, send, recv):
        self.at, self.whole, self.half, self.send, self.recv = place, whole, half, send, recv

    def copy(self, n):
        at = self.at
        if n < 2:
            view, to = self.whole(at.own(0, 0)), at.own(1 - 2 * n, 0)
        elif n < 4:
            view = self.half(at.own(-1 if n == 2 else 1, 0), n - 2)
            to = at.own(1 if n == 2 else -1, 0)
        elif n < 12:
            view = self.whole(at.own(OFFS[n % 4], 0))
            to = at.own(0, 1 if n < 8 else -1)
        elif n < 20:
            low = n < 16
            view = self.half(at.own(OFFS[n % 4], -1 if low else 1), 0 if low else 1)
            to = at.own(0, 1 if low else -1)
        else:
            view = self.whole(at.own(OFFS[n % 4], (0, -1, 1, 2)[(n - 20) // 4]))
            to = at.other(0, 0)
        return remote(view, self.send, self.recv.at[n], (to, at.x))

    def go(self, *ns):
        for n in ns:
            self.copy(n).start()

    def come(self, *ns):
        for n in ns:
            self.copy(n).wait_recv()

    def event(self, e):
        line, i = e // 4, e % 4
        if e == 1:
            self.come(0)
            self.go(2, 5, 9)
        elif e == 2:
            self.come(1)
            self.go(3, 6, 10)
        elif e == 3:
            self.come(2, 3)
            self.go(7, 11)
        elif line == 1:
            self.come(4 + i)
            self.go(12 + i)
        elif line == 2:
            self.come(8 + i)
            self.go(16 + i)
        else:
            self.come(12 + i, 16 + i)
        self.go(20 + e)

    def own_block(self, e):
        return self.at.own(OFFS[e % 4], (0, -1, 1, 2)[e // 4])

    def other_block(self, e):
        return self.at.other(OFFS[e % 4], (0, -1, 1, 2)[e // 4])

    def shared(self, e):
        self.come(20 + e)

    def drain(self, sent):
        remote(sent, self.send, self.recv.at[0], (self.at.other(0, 0), self.at.x)).wait_send()


class Ring:
    def __init__(self, place, whole, half, send, recv, share):
        self.at, self.whole, self.half = place, whole, half
        self.send, self.recv, self.share = send, recv, share

    def copy(self, n):
        at = self.at
        if n < 2:
            view, to = self.whole(at.x), at.ring(1 - 2 * n)
        elif n < 4:
            view = self.half((at.x + (3 if n == 2 else 1)) % 4, n - 2)
            to = at.ring(1 if n == 2 else -1)
        else:
            view, to = self.whole((at.x + (3, 1, 2)[n - 4]) % 4), (at.other(0, 0), at.x)
        return remote(view, self.send, self.recv.at[n], to)

    def start(self):
        self.copy(0).start()
        self.copy(1).start()

    def relay(self):
        for n in (0, 1):
            self.copy(n).wait_recv()
            self.copy(n + 2).start()
            if self.share:
                self.copy(n + 4).start()

    def last(self):
        self.copy(2).wait_recv()
        self.copy(3).wait_recv()
        if self.share:
            self.copy(6).start()

    def shared(self):
        for n in (4, 5, 6):
            self.copy(n).wait_recv()

    def drain(self, sent):
        remote(sent, self.send, self.recv.at[0], self.at.ring(1)).wait_send()


RECV = (0, 1, 2, 4, 8, 3, 5, 9, 6, 10, 12, 7, 11, 13, 14, 15)
CHIPS = (
    (0, 0), (0, 1), (0, 2), (1, 0), (2, 0), (1, 1), (1, 2), (2, 1),
    (2, 2), (0, 3), (3, 0), (1, 3), (3, 1), (2, 3), (3, 2), (3, 3),
)


LAG = 3


def pick(i, values):
    total = 0
    for k, v in enumerate(values):
        total = total + jnp.where(i == k, v, 0)
    return total


def dispatch(i, jobs, low=0):
    if len(jobs) == 1:
        jobs[0]()
        return
    mid = len(jobs) // 2

    @pl.when(i < low + mid)
    def _():
        dispatch(i, jobs[:mid], low)

    @pl.when(i >= low + mid)
    def _():
        dispatch(i, jobs[mid:], low + mid)


CHUNKS = ((0, 0), (0, 384), (1, 0), (2, 384))


def attend(blocks, q_a, q_b, peak, denom, numer, rows):
    def score(chunk):
        which, at = chunk
        q = q_a if which == 0 else q_b
        found = []
        for kv in blocks:
            key = kv[0:rows, 128 * which : 128 * (which + 1)]
            left = jnp.concatenate([key, key], 1)
            found.append(jnp.dot(left, q[:, at : at + rows], preferred_element_type=F32))
        return found

    coming = score(CHUNKS[0])
    for k, (which, at) in enumerate(CHUNKS):
        scores = coming
        if k + 1 < len(CHUNKS):
            coming = score(CHUNKS[k + 1])
        group = min(which, 1)
        cols = slice(at + 2 * rows * group, at + 2 * rows * group + rows)
        before = peak[0:1, cols]
        fresh = before
        for one in scores:
            fresh = jnp.maximum(fresh, jnp.max(one, axis=0, keepdims=True))
        decay = jnp.exp2(before - fresh)
        weights = [jnp.exp2(one - fresh) for one in scores]
        peak[0:1, cols] = fresh
        total = denom[0:1, cols] * decay
        for one in weights:
            total = total + jnp.sum(one, axis=0, keepdims=True)
        denom[0:1, cols] = total
        value = jnp.concatenate(
            [kv[rows + 128 * group : rows + 128 * (group + 1), :] for kv in blocks], 1
        )
        weights = jnp.concatenate([one.astype(BF16) for one in weights], 0)
        added = jnp.dot(value, weights, preferred_element_type=F32)
        numer[:, cols] = numer[:, cols] * decay + added


def hi_lo(q, scale):
    wide = jnp.transpose(q.astype(F32) * scale)
    high = wide.astype(BF16).astype(F32)
    return high, wide - high


def kernel(
    residual, queries_a, keys_a, values_a, queries_b, keys_b, values_b, lambdas_in, head_gain_in,
    out_a, out_b, norm_gain_in, w_gate, w_up, w_down, out,
    lambdas, head_gain, norm_gain, kv, gu, dn, ow, heads, part, came, passing, res, q_in, v_in, q_a, q_b, peak, denom, numer,
    summed, normed, gates, hidden, square,
    kv_send, kv_recv, gu_send, gu_recv, dn_send, dn_recv, ow_send, ow_recv,
    hd_send, hd_recv, rs_send, rs_recv, ps_recv, load,
):
    at = Place()
    me, x = at.me, at.x
    rows = residual.shape[0]
    depth = w_gate.shape[0]
    share = out.shape[1]
    inner = w_gate.shape[1]

    def local(n, src, dst):
        return pltpu.make_async_copy(src, dst, load.at[n])

    with jax.named_scope("entry"):
        loads = [
            local(0, keys_a, kv.at[me, 0:rows, 0:128]),
            local(1, keys_b, kv.at[me, 0:rows, 128:384]),
            local(2, values_a, v_in.at[0]),
            local(3, values_b, v_in.at[1]),
            local(4, queries_a, q_in.at[:, 0:128]),
            local(5, queries_b, q_in.at[:, 128:384]),
            local(6, out_a, ow.at[x, 0]),
            local(7, out_b, ow.at[x, 1]),
            local(8, w_gate, gu.at[0, me]),
            local(9, w_up, gu.at[1, me]),
            local(10, w_down, dn.at[me]),
            local(11, residual, res),
            local(12, lambdas_in, lambdas),
            local(13, head_gain_in, head_gain),
            local(14, norm_gain_in, norm_gain),
        ]
        for c in loads[:6]:
            c.start()

        barrier = pltpu.get_barrier_semaphore()
        friends = [(at.own(1, 0), x), (at.own(-1, 0), x), (at.own(0, 1), x), (at.own(0, -1), x)]
        friends += [(at.other(0, 0), x), at.ring(1), at.ring(2), at.ring(-1)]
        for f in friends:
            pl.semaphore_signal(barrier, inc=1, device_id=f, device_id_type=MESH)

        for n in (2, 3):
            loads[n].wait()
        for g in range(2):
            kv[me, rows + 128 * g : rows + 128 * (g + 1), :] = jnp.transpose(
                v_in[g].astype(F32)
            ).astype(BF16)
        for n in (0, 1):
            loads[n].wait()
        pl.semaphore_wait(barrier, len(friends))

    cut = (rows + 256) // 2
    KV = Plane(
        at, lambda b: kv.at[b], lambda b, h: kv.at[b, cut * h : cut * (h + 1)], kv_send, kv_recv
    )
    mid = depth // 2
    GU = Plane(
        at,
        lambda b: gu.at[:, b],
        lambda b, h: gu.at[:, b, mid * h : mid * (h + 1)],
        gu_send,
        gu_recv,
    )
    DN = Plane(
        at, lambda b: dn.at[b], lambda b, h: dn.at[b, mid * h : mid * (h + 1)], dn_send, dn_recv
    )
    OW = Ring(
        at,
        lambda b: ow.at[b, at.c],
        lambda b, h: ow.at[b, at.c, 64 * h : 64 * (h + 1)],
        ow_send,
        ow_recv,
        True,
    )
    HD = Ring(
        at,
        lambda b: heads.at[b],
        lambda b, h: heads.at[b, rows // 2 * h : rows // 2 * (h + 1)],
        hd_send,
        hd_recv,
        False,
    )
    with jax.named_scope("prep"):
        KV.go(0, 1, 4, 8, 20)
        for c in loads[6:]:
            c.start()
        for n in (6, 7):
            loads[n].wait()
        OW.start()

        for n in (4, 5):
            loads[n].wait()
        high, low = hi_lo(q_in[:, 0:128], log2e / 8.0)
        first = lax.broadcasted_iota(jnp.int32, high.shape, 0) < 64
        for j in range(2):
            keep = first if j == 0 else jnp.logical_not(first)
            cols = slice(rows * j, rows * (j + 1))
            q_a[0:128, cols] = jnp.where(keep, high, 0.0).astype(BF16)
            q_a[128:256, cols] = jnp.where(keep, low, 0.0).astype(BF16)
            high_b, low_b = hi_lo(q_in[:, 128 * (j + 1) : 128 * (j + 2)], log2e * 128.0**-0.5)
            q_b[0:128, cols] = high_b.astype(BF16)
            q_b[128:256, cols] = low_b.astype(BF16)
        peak[...] = jnp.full(peak.shape, -1e30, F32)
        denom[...] = jnp.zeros(denom.shape, F32)
        numer[...] = jnp.zeros(numer.shape, F32)
        for n in range(8, 15):
            loads[n].wait()

    def take(k):
        def job():
            if k == 1:
                KV.event(RECV[1])
            if 1 <= k < 15:
                KV.event(RECV[k + 1])
            if k == 11:
                GU.go(4, 8, 20)
            if k == 12:
                GU.go(0, 1)
            KV.shared(RECV[k])
            if k == 5:
                OW.relay()
            if k == 10:
                OW.last()

        return job

    turns = [(OFFS[e % 4] + 4) % 4 for e in RECV]
    lines = [(OFFS[e // 4] + 4) % 4 for e in RECV]

    def step(i, carry):
        with jax.named_scope("take"):
            dispatch(i, [take(k) for k in range(16)])
            dp, ds = pick(i, turns), pick(i, lines)
            blocks = [kv.at[at.own(dp, ds)], kv.at[at.other(dp, ds)]]
        with jax.named_scope("attend"):
            attend(blocks, q_a, q_b, peak, denom, numer, rows)
        return carry

    lax.fori_loop(0, 16, step, 0)

    with jax.named_scope("gu_one"):
        GU.event(1)
        GU.event(2)

    with jax.named_scope("finish"):
        ratio = numer[...] / denom[0:1, :]
        for g in range(2):
            base = 2 * rows * g
            mixed = ratio[:, base : base + rows] - lambdas[0, g] * ratio[:, base + rows : base + 2 * rows]
            scale = lax.rsqrt(jnp.mean(mixed * mixed, axis=0, keepdims=True) + eps_norm)
            done = jnp.transpose(mixed * scale) * head_gain[g : g + 1, :] * head_scale
            heads[x, :, 128 * g : 128 * (g + 1)] = done.astype(BF16)
        HD.start()

    with jax.named_scope("gu_two"):
        GU.event(4)
        GU.event(8)
    with jax.named_scope("hd_relay"):
        HD.relay()
    with jax.named_scope("gu_2b"):
        for e in (3, 5, 9):
            GU.event(e)
    with jax.named_scope("hd_last"):
        HD.last()
        OW.shared()
        wide = summed.shape[1]

    with jax.named_scope("project"):
        square[...] = jnp.zeros(square.shape, F32)

        @pl.loop(0, wide // 256)
        def _(n):
            cols = pl.ds(pl.multiple_of(n * 256, 256), 256)
            left = jnp.concatenate([heads[k] for k in range(4)], axis=1)
            right = ow[:, :, :, cols].reshape(1024, 256)
            total = res[:, cols].astype(F32) + jnp.dot(left, right, preferred_element_type=F32)
            summed[:, cols] = total
            twice = total * total
            square[...] += twice[:, 0:128] + twice[:, 128:256]

    with jax.named_scope("gu_three"):
        for e in (6, 10, 12):
            GU.event(e)

    with jax.named_scope("norm"):
        inverse = lax.rsqrt(jnp.sum(square[...], axis=1, keepdims=True) / wide + eps_norm)

        @pl.loop(0, wide // 256)
        def _(n):
            cols = pl.ds(pl.multiple_of(n * 256, 256), 256)
            normed[:, cols] = (summed[:, cols] * inverse * norm_gain[0:1, cols]).astype(BF16)

    pieces = ((0, 512), (512, 512), (1024, inner - 1024))
    with jax.named_scope("gu_four"):
        gates[...] = jnp.zeros(gates.shape, F32)
        KV.drain(kv.at[0:31])
        OW.drain(ow.at[0:3])
        HD.drain(heads.at[0:3])

    def line(k):
        def job():
            if k == 1:
                GU.event(7)
                GU.event(11)
                DN.go(4, 8, 20, 0, 1)
            if k > 0:
                GU.event(12 + k)
            if k == 3:
                DN.event(1)
                DN.event(2)
            for other in range(4):
                GU.shared(4 * other + k)

        return job

    def gate_step(k, carry):
        with jax.named_scope("line"):
            dispatch(k, [line(n) for n in range(4)])
            s = (at.s + pick(k, (0, 3, 1, 2))) % 4
            chips = [(1 - at.c) * (4 * s + n) + at.c * (4 * n + s) for n in range(4)]
        with jax.named_scope("gate"):
            left = jnp.concatenate(
                [normed[:, pl.ds(pl.multiple_of(n * 128, 128), 128)] for n in chips], axis=1
            )
            for g in range(2):
                for lo, n in pieces:
                    right = jnp.concatenate(
                        [gu[g, pl.ds(2 * m, 2), :, lo : lo + n].reshape(128, n) for m in chips],
                        axis=0,
                    )
                    gates[g, :, lo : lo + n] += jnp.dot(left, right, preferred_element_type=F32)
        return carry

    lax.fori_loop(0, 4, gate_step, 0)

    with jax.named_scope("act"):
        for lo, n in pieces:
            gate = gates[0, :, lo : lo + n]
            hidden[:, lo : lo + n] = (
                gate / (1.0 + jnp.exp(-gate)) * gates[1, :, lo : lo + n]
            ).astype(BF16)

    with jax.named_scope("dn_one"):
        DN.event(4)
        DN.event(8)
        GU.drain(gu.at[:, 0:31])

    half = rows // 2

    def give(chip, h, to, target, arrived):
        return pltpu.make_async_remote_copy(
            src_ref=part.at[chip, half * h : half * (h + 1)],
            dst_ref=target,
            send_sem=rs_send,
            recv_sem=arrived,
            device_id=(me, to),
            device_id_type=MESH,
        )

    def side(chip, n, h):
        y = chip % 4
        target = came.at[n, y, half * h : half * (h + 1)]
        return give(chip, h, chip // 4, target, rs_recv.at[8 * n + 2 * y + h])

    def through(chip, n):
        y = chip % 4
        return give(chip, n, (x + 1 + 2 * n) % 4, passing.at[n, y], ps_recv.at[4 * n + y])

    def first_give(chip):
        away = (chip // 4 - x + 4) % 4

        @pl.when(away == 2)
        def _():
            through(chip, 0).start()
            through(chip, 1).start()

        for n in range(2):

            @pl.when(away == 1 + 2 * n)
            def _(n=n):
                side(chip, n, 1 - n).start()

    def second_give(chip):
        y = chip % 4
        away = (chip // 4 - x + 4) % 4
        for n in range(2):

            @pl.when(away == 1 + 2 * n)
            def _(n=n):
                through(chip, n).wait_recv()
                mine = part[chip, half * n : half * (n + 1)].astype(F32)
                mine = mine + passing[n, y].astype(F32)
                part[chip, half * n : half * (n + 1)] = mine.astype(BF16)
                side(chip, n, n).start()

    down_events = ((), (), (3, 5, 9), (6, 10), (12,), (7, 11, 13), (14,), (15,))
    down_shared = ((0, 1), (2, 4), (8, 5), (6, 9), (10, 3), (12, 7), (13, 11), (14, 15))

    def arrive(k):
        def job():
            for e in down_events[k]:
                DN.event(e)
            for e in down_shared[k]:
                DN.shared(e)

        return job

    offsets = (0, 3, 1, 2)

    def chips_of(k):
        found = []
        for n in range(2):
            dp = pick(k, [offsets[a] for a, _ in CHIPS[n::2]])
            ds = pick(k, [offsets[b] for _, b in CHIPS[n::2]])
            found.append(at.own(dp, ds) // 2)
        return found

    def down_step(k, carry):
        with jax.named_scope("arrive"):
            dispatch(k, [arrive(n) for n in range(8)])
            chips = chips_of(k)
        with jax.named_scope("down"):
            right = jnp.concatenate(
                [dn[pl.ds(2 * m, 2)].reshape(128, inner) for m in chips], axis=0
            )
            sums = lax.dot_general(
                hidden[...], right, (((1,), (1,)), ((), ())), preferred_element_type=F32
            ).astype(BF16)
            for n, m in enumerate(chips):
                part[m] = sums[:, 128 * n : 128 * (n + 1)]
        with jax.named_scope("give"):
            for m in chips:
                first_give(m)

        with jax.named_scope("second"):

            @pl.when(k >= LAG)
            def _():
                for m in chips_of(k - LAG):
                    second_give(m)

        return carry

    lax.fori_loop(0, 8, down_step, 0)

    with jax.named_scope("late"):

        @pl.loop(8 - LAG, 8)
        def _(k):
            for m in chips_of(k):
                second_give(m)

    with jax.named_scope("sum"):

        def sum_step(k, carry):
            for m in chips_of(k):

                @pl.when(m // 4 == x)
                def _(m=m):
                    y = m % 4
                    cols = pl.ds(pl.multiple_of(x * share + 128 * y, 128), 128)
                    into = pl.ds(pl.multiple_of(128 * y, 128), 128)
                    for n in range(2):
                        for h in range(2):
                            side(m, n, h).wait_recv()
                    total = (
                        part[m].astype(F32) + came[0, y].astype(F32) + came[1, y].astype(F32)
                    )
                    out[:, into] = (summed[:, cols] + 0.5 * total).astype(BF16)

            return carry

        lax.fori_loop(0, 8, sum_step, 0)

    with jax.named_scope("drain"):
        DN.drain(dn.at[0:31])
        remote(part.at[0:12], rs_send, rs_recv.at[0], at.ring(1)).wait_send()


def local(
    residual, queries_a, keys_a, values_a, queries_b, keys_b, values_b, mix_lambda, head_gain,
    out_a, out_b, norm_gain, w_gate, w_up, w_down,
):
    rows, wide = residual.shape
    depth, inner = w_gate.shape
    share = wide // 4
    anywhere = pl.BlockSpec(memory_space=pl.ANY)
    dma = pltpu.SemaphoreType.DMA
    count = Plane.count
    return pl.pallas_call(
        kernel,
        out_shape=pltpu.VMEM((rows, share), BF16),
        in_specs=[anywhere] * 15,
        out_specs=pl.BlockSpec(memory_space=pltpu.VMEM),
        scratch_shapes=[
            pltpu.SMEM((1, 2), F32),
            pltpu.VMEM((2, 128), F32),
            pltpu.VMEM((1, wide), F32),
            pltpu.VMEM((32, rows + 256, rows), BF16),
            pltpu.VMEM((2, 32, depth, inner), BF16),
            pltpu.VMEM((32, depth, inner), BF16),
            pltpu.VMEM((4, 2, 128, wide), BF16),
            pltpu.VMEM((4, rows, 256), BF16),
            pltpu.VMEM((16, rows, 128), BF16),
            pltpu.VMEM((2, 4, rows, 128), BF16),
            pltpu.VMEM((2, 4, rows // 2, 128), BF16),
            pltpu.VMEM((rows, wide), BF16),
            pltpu.VMEM((rows, 384), BF16),
            pltpu.VMEM((2, rows, 128), BF16),
            pltpu.VMEM((256, 2 * rows), BF16),
            pltpu.VMEM((256, 2 * rows), BF16),
            pltpu.VMEM((1, 4 * rows), F32),
            pltpu.VMEM((1, 4 * rows), F32),
            pltpu.VMEM((128, 4 * rows), F32),
            pltpu.VMEM((rows, wide), F32),
            pltpu.VMEM((rows, wide), BF16),
            pltpu.VMEM((2, rows, inner), F32),
            pltpu.VMEM((rows, inner), BF16),
            pltpu.VMEM((rows, 128), F32),
            dma, dma((count,)), dma, dma((count,)), dma, dma((count,)),
            dma, dma((7,)), dma, dma((4,)), dma, dma((16,)), dma((8,)),
            dma((15,)),
        ],
        compiler_params=pltpu.CompilerParams(
            collective_id=0, has_side_effects=True, vmem_limit_bytes=66 * 1000 * 1000
        ),
        name="layer",
    )(
        residual, queries_a, keys_a, values_a, queries_b, keys_b, values_b, mix_lambda.T, head_gain,
        out_a, out_b, norm_gain.reshape(1, wide), w_gate, w_up, w_down.T,
    )


def solution(mesh):
    in_specs = (
        P("sp", None),
        P("sp", "tp"),
        P("sp", "tp"),
        P("sp", "tp"),
        P("sp", "tp"),
        P("sp", "tp"),
        P("sp", "tp"),
        P(None, "tp"),
        P(),
        P("tp", None),
        P("tp", None),
        P(),
        P("sp", "tp"),
        P("sp", "tp"),
        P("tp", "sp"),
    )
    return jax.shard_map(
        local, mesh=mesh, in_specs=in_specs, out_specs=P("sp", "tp"), check_vma=False
    )
```

```python
import functools

import jax
import jax.numpy as jnp
from jax import lax
from jax.experimental import pallas as pl
from jax.experimental.pallas import tpu as pltpu
from jax.sharding import PartitionSpec as P

MESH = pl.DeviceIdType.MESH
F32 = jnp.float32
BF16 = jnp.bfloat16
eps_norm = 1e-06
head_scale = 0.8
log2e = 1.4426950408889634
OFFS = (0, -1, 1, 2)


class Place:
    def __init__(self):
        self.x = lax.axis_index("tp")
        self.me = lax.axis_index("sp")
        self.c = self.me % 2
        y = (self.me // 2) % 4
        z = self.me // 8
        self.z = z
        self.p = y * (1 - self.c) + z * self.c
        self.s = z * (1 - self.c) + y * self.c

    def own(self, dp, ds):
        p, s, c = (self.p + dp + 4) % 4, (self.s + ds + 4) % 4, self.c
        return ((1 - c) * (4 * s + p) + c * (4 * p + s)) * 2 + c

    def other(self, dp, ds):
        p, s, c = (self.s + dp + 4) % 4, (self.p + ds + 4) % 4, 1 - self.c
        return ((1 - c) * (4 * s + p) + c * (4 * p + s)) * 2 + c

    def ring(self, dx):
        return (self.me, (self.x + dx + 4) % 4)


def remote(view, send, recv, device):
    return pltpu.make_async_remote_copy(
        src_ref=view,
        dst_ref=view,
        send_sem=send,
        recv_sem=recv,
        device_id=device,
        device_id_type=MESH,
    )


class Plane:
    count = 36

    def __init__(self, place, whole, half, send, recv):
        self.at, self.whole, self.half, self.send, self.recv = place, whole, half, send, recv

    def copy(self, n):
        at = self.at
        if n < 2:
            view, to = self.whole(at.own(0, 0)), at.own(1 - 2 * n, 0)
        elif n < 4:
            view = self.half(at.own(-1 if n == 2 else 1, 0), n - 2)
            to = at.own(1 if n == 2 else -1, 0)
        elif n < 12:
            view = self.whole(at.own(OFFS[n % 4], 0))
            to = at.own(0, 1 if n < 8 else -1)
        elif n < 20:
            low = n < 16
            view = self.half(at.own(OFFS[n % 4], -1 if low else 1), 0 if low else 1)
            to = at.own(0, 1 if low else -1)
        else:
            view = self.whole(at.own(OFFS[n % 4], (0, -1, 1, 2)[(n - 20) // 4]))
            to = at.other(0, 0)
        return remote(view, self.send, self.recv.at[n], (to, at.x))

    def go(self, *ns):
        for n in ns:
            self.copy(n).start()

    def come(self, *ns):
        for n in ns:
            self.copy(n).wait_recv()

    def event(self, e):
        line, i = e // 4, e % 4
        if e == 1:
            self.come(0)
            self.go(2, 5, 9)
        elif e == 2:
            self.come(1)
            self.go(3, 6, 10)
        elif e == 3:
            self.come(2, 3)
            self.go(7, 11)
        elif line == 1:
            self.come(4 + i)
            self.go(12 + i)
        elif line == 2:
            self.come(8 + i)
            self.go(16 + i)
        else:
            self.come(12 + i, 16 + i)
        self.go(20 + e)

    def own_block(self, e):
        return self.at.own(OFFS[e % 4], (0, -1, 1, 2)[e // 4])

    def other_block(self, e):
        return self.at.other(OFFS[e % 4], (0, -1, 1, 2)[e // 4])

    def shared(self, e):
        self.come(20 + e)

    def drain(self, sent):
        remote(sent, self.send, self.recv.at[0], (self.at.other(0, 0), self.at.x)).wait_send()


class Ring:
    def __init__(self, place, whole, half, send, recv, share):
        self.at, self.whole, self.half = place, whole, half
        self.send, self.recv, self.share = send, recv, share

    def copy(self, n):
        at = self.at
        if n < 2:
            view, to = self.whole(at.x), at.ring(1 - 2 * n)
        elif n < 4:
            view = self.half((at.x + (3 if n == 2 else 1)) % 4, n - 2)
            to = at.ring(1 if n == 2 else -1)
        else:
            view, to = self.whole((at.x + (3, 1, 2)[n - 4]) % 4), (at.other(0, 0), at.x)
        return remote(view, self.send, self.recv.at[n], to)

    def start(self):
        self.copy(0).start()
        self.copy(1).start()

    def relay(self):
        for n in (0, 1):
            self.copy(n).wait_recv()
            self.copy(n + 2).start()
            if self.share:
                self.copy(n + 4).start()

    def last(self):
        self.copy(2).wait_recv()
        self.copy(3).wait_recv()
        if self.share:
            self.copy(6).start()

    def shared(self):
        for n in (4, 5, 6):
            self.copy(n).wait_recv()

    def drain(self, sent):
        remote(sent, self.send, self.recv.at[0], self.at.ring(1)).wait_send()


RECV = (0, 1, 2, 4, 8, 3, 5, 9, 6, 10, 12, 7, 11, 13, 14, 15)
CHIPS = (
    (0, 0), (0, 1), (0, 2), (1, 0), (2, 0), (1, 1), (1, 2), (2, 1),
    (2, 2), (0, 3), (3, 0), (1, 3), (3, 1), (2, 3), (3, 2), (3, 3),
)


LAG = 3


def pick(i, values):
    total = 0
    for k, v in enumerate(values):
        total = total + jnp.where(i == k, v, 0)
    return total


def dispatch(i, jobs, low=0):
    if len(jobs) == 1:
        jobs[0]()
        return
    mid = len(jobs) // 2

    @pl.when(i < low + mid)
    def _():
        dispatch(i, jobs[:mid], low)

    @pl.when(i >= low + mid)
    def _():
        dispatch(i, jobs[mid:], low + mid)


CHUNKS = ((0, 0), (0, 384), (1, 0), (2, 384))


def attend(blocks, q_a, q_b, peak, denom, numer, rows):
    def score(chunk):
        which, at = chunk
        q = q_a if which == 0 else q_b
        found = []
        for kv in blocks:
            key = kv[0:rows, 128 * which : 128 * (which + 1)]
            left = jnp.concatenate([key, key], 1)
            found.append(jnp.dot(left, q[:, at : at + rows], preferred_element_type=F32))
        return found

    coming = score(CHUNKS[0])
    for k, (which, at) in enumerate(CHUNKS):
        scores = coming
        if k + 1 < len(CHUNKS):
            coming = score(CHUNKS[k + 1])
        group = min(which, 1)
        cols = slice(at + 2 * rows * group, at + 2 * rows * group + rows)
        before = peak[0:1, cols]
        fresh = before
        for one in scores:
            fresh = jnp.maximum(fresh, jnp.max(one, axis=0, keepdims=True))
        decay = jnp.exp2(before - fresh)
        weights = [jnp.exp2(one - fresh) for one in scores]
        peak[0:1, cols] = fresh
        total = denom[0:1, cols] * decay
        for one in weights:
            total = total + jnp.sum(one, axis=0, keepdims=True)
        denom[0:1, cols] = total
        value = jnp.concatenate(
            [kv[rows + 128 * group : rows + 128 * (group + 1), :] for kv in blocks], 1
        )
        weights = jnp.concatenate([one.astype(BF16) for one in weights], 0)
        added = jnp.dot(value, weights, preferred_element_type=F32)
        numer[:, cols] = numer[:, cols] * decay + added


def hi_lo(q, scale):
    wide = jnp.transpose(q.astype(F32) * scale)
    high = wide.astype(BF16).astype(F32)
    return high, wide - high


def kernel(
    residual, queries_a, keys_a, values_a, queries_b, keys_b, values_b, lambdas_in, head_gain_in,
    out_a, out_b, norm_gain_in, w_gate, w_up, w_down, out,
    lambdas, head_gain, norm_gain, kv, gu, dn, ow, heads, part, came, passing, res, q_in, v_in, q_a, q_b, peak, denom, numer,
    summed, normed, gates, hidden, square,
    kv_send, kv_recv, gu_send, gu_recv, dn_send, dn_recv, ow_send, ow_recv,
    hd_send, hd_recv, rs_send, rs_recv, ps_recv, load,
):
    at = Place()
    me, x = at.me, at.x
    rows = residual.shape[0]
    depth = w_gate.shape[0]
    share = out.shape[1]
    inner = w_gate.shape[1]

    def local(n, src, dst):
        return pltpu.make_async_copy(src, dst, load.at[n])

    with jax.named_scope("entry"):
        loads = [
            local(0, keys_a, kv.at[me, 0:rows, 0:128]),
            local(1, keys_b, kv.at[me, 0:rows, 128:384]),
            local(2, values_a, v_in.at[0]),
            local(3, values_b, v_in.at[1]),
            local(4, queries_a, q_in.at[:, 0:128]),
            local(5, queries_b, q_in.at[:, 128:384]),
            local(6, out_a, ow.at[x, 0]),
            local(7, out_b, ow.at[x, 1]),
            local(8, w_gate, gu.at[0, me]),
            local(9, w_up, gu.at[1, me]),
            local(10, w_down, dn.at[me]),
            local(11, residual, res),
            local(12, lambdas_in, lambdas),
            local(13, head_gain_in, head_gain),
            local(14, norm_gain_in, norm_gain),
        ]
        for c in loads[:6]:
            c.start()

        barrier = pltpu.get_barrier_semaphore()
        friends = [(at.own(1, 0), x), (at.own(-1, 0), x), (at.own(0, 1), x), (at.own(0, -1), x)]
        friends += [(at.other(0, 0), x), at.ring(1), at.ring(2), at.ring(-1)]
        for f in friends:
            pl.semaphore_signal(barrier, inc=1, device_id=f, device_id_type=MESH)

        for n in (2, 3):
            loads[n].wait()
        for g in range(2):
            kv[me, rows + 128 * g : rows + 128 * (g + 1), :] = jnp.transpose(
                v_in[g].astype(F32)
            ).astype(BF16)
        for n in (0, 1):
            loads[n].wait()
        pl.semaphore_wait(barrier, len(friends))

    cut = (rows + 256) // 2
    KV = Plane(
        at, lambda b: kv.at[b], lambda b, h: kv.at[b, cut * h : cut * (h + 1)], kv_send, kv_recv
    )
    mid = depth // 2
    GU = Plane(
        at,
        lambda b: gu.at[:, b],
        lambda b, h: gu.at[:, b, mid * h : mid * (h + 1)],
        gu_send,
        gu_recv,
    )
    DN = Plane(
        at, lambda b: dn.at[b], lambda b, h: dn.at[b, mid * h : mid * (h + 1)], dn_send, dn_recv
    )
    OW = Ring(
        at,
        lambda b: ow.at[b, at.c],
        lambda b, h: ow.at[b, at.c, 64 * h : 64 * (h + 1)],
        ow_send,
        ow_recv,
        True,
    )
    HD = Ring(
        at,
        lambda b: heads.at[b],
        lambda b, h: heads.at[b, rows // 2 * h : rows // 2 * (h + 1)],
        hd_send,
        hd_recv,
        False,
    )
    with jax.named_scope("prep"):
        KV.go(0, 1, 4, 8, 20)
        for c in loads[6:]:
            c.start()
        for n in (6, 7):
            loads[n].wait()
        OW.start()

        for n in (4, 5):
            loads[n].wait()
        high, low = hi_lo(q_in[:, 0:128], log2e / 8.0)
        first = lax.broadcasted_iota(jnp.int32, high.shape, 0) < 64
        for j in range(2):
            keep = first if j == 0 else jnp.logical_not(first)
            cols = slice(rows * j, rows * (j + 1))
            q_a[0:128, cols] = jnp.where(keep, high, 0.0).astype(BF16)
            q_a[128:256, cols] = jnp.where(keep, low, 0.0).astype(BF16)
            high_b, low_b = hi_lo(q_in[:, 128 * (j + 1) : 128 * (j + 2)], log2e * 128.0**-0.5)
            q_b[0:128, cols] = high_b.astype(BF16)
            q_b[128:256, cols] = low_b.astype(BF16)
        peak[...] = jnp.full(peak.shape, -1e30, F32)
        denom[...] = jnp.zeros(denom.shape, F32)
        numer[...] = jnp.zeros(numer.shape, F32)
        for n in range(8, 15):
            loads[n].wait()

    def take(k):
        def job():
            if k == 1:
                KV.event(RECV[1])
            if 1 <= k < 15:
                KV.event(RECV[k + 1])
            if k == 12:
                GU.go(0, 1, 4, 8, 20)
            KV.shared(RECV[k])
            if k == 5:
                OW.relay()
            if k == 10:
                OW.last()

        return job

    turns = [(OFFS[e % 4] + 4) % 4 for e in RECV]
    lines = [(OFFS[e // 4] + 4) % 4 for e in RECV]

    def step(i, carry):
        with jax.named_scope("take"):
            dispatch(i, [take(k) for k in range(16)])
            dp, ds = pick(i, turns), pick(i, lines)
            blocks = [kv.at[at.own(dp, ds)], kv.at[at.other(dp, ds)]]
        with jax.named_scope("attend"):
            attend(blocks, q_a, q_b, peak, denom, numer, rows)
        return carry

    lax.fori_loop(0, 16, step, 0)

    with jax.named_scope("gu_one"):
        GU.event(1)
        GU.event(2)

    with jax.named_scope("finish"):
        ratio = numer[...] / denom[0:1, :]
        for g in range(2):
            base = 2 * rows * g
            mixed = ratio[:, base : base + rows] - lambdas[0, g] * ratio[:, base + rows : base + 2 * rows]
            scale = lax.rsqrt(jnp.mean(mixed * mixed, axis=0, keepdims=True) + eps_norm)
            done = jnp.transpose(mixed * scale) * head_gain[g : g + 1, :] * head_scale
            heads[x, :, 128 * g : 128 * (g + 1)] = done.astype(BF16)
        HD.start()

    with jax.named_scope("gu_two"):
        GU.event(4)
        GU.event(8)
    with jax.named_scope("hd_relay"):
        HD.relay()
    with jax.named_scope("gu_2b"):
        for e in (3, 5, 9):
            GU.event(e)
    with jax.named_scope("hd_last"):
        HD.last()
        OW.shared()
        wide = summed.shape[1]

    with jax.named_scope("project"):
        square[...] = jnp.zeros(square.shape, F32)

        @pl.loop(0, wide // 256)
        def _(n):
            cols = pl.ds(pl.multiple_of(n * 256, 256), 256)
            left = jnp.concatenate([heads[k] for k in range(4)], axis=1)
            right = ow[:, :, :, cols].reshape(1024, 256)
            total = res[:, cols].astype(F32) + jnp.dot(left, right, preferred_element_type=F32)
            summed[:, cols] = total
            twice = total * total
            square[...] += twice[:, 0:128] + twice[:, 128:256]

    with jax.named_scope("gu_three"):
        for e in (6, 10, 12):
            GU.event(e)

    with jax.named_scope("norm"):
        inverse = lax.rsqrt(jnp.sum(square[...], axis=1, keepdims=True) / wide + eps_norm)

        @pl.loop(0, wide // 256)
        def _(n):
            cols = pl.ds(pl.multiple_of(n * 256, 256), 256)
            normed[:, cols] = (summed[:, cols] * inverse * norm_gain[0:1, cols]).astype(BF16)

    pieces = ((0, 512), (512, 512), (1024, inner - 1024))
    with jax.named_scope("gu_four"):
        gates[...] = jnp.zeros(gates.shape, F32)
        KV.drain(kv.at[0:31])
        OW.drain(ow.at[0:3])
        HD.drain(heads.at[0:3])

    def line(k):
        def job():
            if k == 1:
                GU.event(7)
                GU.event(11)
                DN.go(0, 1, 4, 8, 20)
            if k > 0:
                GU.event(12 + k)
            if k == 3:
                DN.event(1)
                DN.event(2)
            for other in range(4):
                GU.shared(4 * other + k)

        return job

    def gate_step(k, carry):
        with jax.named_scope("line"):
            dispatch(k, [line(n) for n in range(4)])
            s = (at.s + pick(k, (0, 3, 1, 2))) % 4
            chips = [(1 - at.c) * (4 * s + n) + at.c * (4 * n + s) for n in range(4)]
        with jax.named_scope("gate"):
            left = jnp.concatenate(
                [normed[:, pl.ds(pl.multiple_of(n * 128, 128), 128)] for n in chips], axis=1
            )
            for g in range(2):
                for lo, n in pieces:
                    right = jnp.concatenate(
                        [gu[g, pl.ds(2 * m, 2), :, lo : lo + n].reshape(128, n) for m in chips],
                        axis=0,
                    )
                    gates[g, :, lo : lo + n] += jnp.dot(left, right, preferred_element_type=F32)
        return carry

    lax.fori_loop(0, 4, gate_step, 0)

    with jax.named_scope("act"):
        for lo, n in pieces:
            gate = gates[0, :, lo : lo + n]
            hidden[:, lo : lo + n] = (
                gate / (1.0 + jnp.exp(-gate)) * gates[1, :, lo : lo + n]
            ).astype(BF16)

    with jax.named_scope("dn_one"):
        DN.event(4)
        DN.event(8)
        GU.drain(gu.at[:, 0:31])

    half = rows // 2

    def give(chip, h, to, target, arrived):
        return pltpu.make_async_remote_copy(
            src_ref=part.at[chip, half * h : half * (h + 1)],
            dst_ref=target,
            send_sem=rs_send,
            recv_sem=arrived,
            device_id=(me, to),
            device_id_type=MESH,
        )

    def side(chip, n, h):
        y = chip % 4
        target = came.at[n, y, half * h : half * (h + 1)]
        return give(chip, h, chip // 4, target, rs_recv.at[8 * n + 2 * y + h])

    def through(chip, n):
        y = chip % 4
        return give(chip, n, (x + 1 + 2 * n) % 4, passing.at[n, y], ps_recv.at[4 * n + y])

    def first_give(chip):
        away = (chip // 4 - x + 4) % 4

        @pl.when(away == 2)
        def _():
            through(chip, 0).start()
            through(chip, 1).start()

        for n in range(2):

            @pl.when(away == 1 + 2 * n)
            def _(n=n):
                side(chip, n, 1 - n).start()

    def second_give(chip):
        y = chip % 4
        away = (chip // 4 - x + 4) % 4
        for n in range(2):

            @pl.when(away == 1 + 2 * n)
            def _(n=n):
                through(chip, n).wait_recv()
                mine = part[chip, half * n : half * (n + 1)].astype(F32)
                mine = mine + passing[n, y].astype(F32)
                part[chip, half * n : half * (n + 1)] = mine.astype(BF16)
                side(chip, n, n).start()

    down_events = ((), (), (3, 5, 9), (6, 10), (12,), (7, 11, 13), (14,), (15,))
    down_shared = ((0, 1), (2, 4), (8, 5), (6, 9), (10, 3), (12, 7), (13, 11), (14, 15))

    def arrive(k):
        def job():
            for e in down_events[k]:
                DN.event(e)
            for e in down_shared[k]:
                DN.shared(e)

        return job

    offsets = (0, 3, 1, 2)

    def chips_of(k):
        found = []
        for n in range(2):
            dp = pick(k, [offsets[a] for a, _ in CHIPS[n::2]])
            ds = pick(k, [offsets[b] for _, b in CHIPS[n::2]])
            found.append(at.own(dp, ds) // 2)
        return found

    def down_step(k, carry):
        with jax.named_scope("arrive"):
            dispatch(k, [arrive(n) for n in range(8)])
            chips = chips_of(k)
        with jax.named_scope("down"):
            right = jnp.concatenate(
                [dn[pl.ds(2 * m, 2)].reshape(128, inner) for m in chips], axis=0
            )
            sums = lax.dot_general(
                hidden[...], right, (((1,), (1,)), ((), ())), preferred_element_type=F32
            ).astype(BF16)
            for n, m in enumerate(chips):
                part[m] = sums[:, 128 * n : 128 * (n + 1)]
        with jax.named_scope("give"):
            for m in chips:
                first_give(m)

        with jax.named_scope("second"):

            @pl.when(k >= LAG)
            def _():
                for m in chips_of(k - LAG):
                    second_give(m)

        return carry

    lax.fori_loop(0, 8, down_step, 0)

    with jax.named_scope("late"):

        @pl.loop(8 - LAG, 8)
        def _(k):
            for m in chips_of(k):
                second_give(m)

    with jax.named_scope("sum"):

        def sum_step(k, carry):
            for m in chips_of(k):

                @pl.when(m // 4 == x)
                def _(m=m):
                    y = m % 4
                    cols = pl.ds(pl.multiple_of(x * share + 128 * y, 128), 128)
                    into = pl.ds(pl.multiple_of(128 * y, 128), 128)
                    for n in range(2):
                        for h in range(2):
                            side(m, n, h).wait_recv()
                    total = (
                        part[m].astype(F32) + came[0, y].astype(F32) + came[1, y].astype(F32)
                    )
                    out[:, into] = (summed[:, cols] + 0.5 * total).astype(BF16)

            return carry

        lax.fori_loop(0, 8, sum_step, 0)

    with jax.named_scope("drain"):
        DN.drain(dn.at[0:31])
        remote(part.at[0:12], rs_send, rs_recv.at[0], at.ring(1)).wait_send()


def local(
    residual, queries_a, keys_a, values_a, queries_b, keys_b, values_b, mix_lambda, head_gain,
    out_a, out_b, norm_gain, w_gate, w_up, w_down,
):
    rows, wide = residual.shape
    depth, inner = w_gate.shape
    share = wide // 4
    anywhere = pl.BlockSpec(memory_space=pl.ANY)
    dma = pltpu.SemaphoreType.DMA
    count = Plane.count
    return pl.pallas_call(
        kernel,
        out_shape=pltpu.VMEM((rows, share), BF16),
        in_specs=[anywhere] * 15,
        out_specs=pl.BlockSpec(memory_space=pltpu.VMEM),
        scratch_shapes=[
            pltpu.SMEM((1, 2), F32),
            pltpu.VMEM((2, 128), F32),
            pltpu.VMEM((1, wide), F32),
            pltpu.VMEM((32, rows + 256, rows), BF16),
            pltpu.VMEM((2, 32, depth, inner), BF16),
            pltpu.VMEM((32, depth, inner), BF16),
            pltpu.VMEM((4, 2, 128, wide), BF16),
            pltpu.VMEM((4, rows, 256), BF16),
            pltpu.VMEM((16, rows, 128), BF16),
            pltpu.VMEM((2, 4, rows, 128), BF16),
            pltpu.VMEM((2, 4, rows // 2, 128), BF16),
            pltpu.VMEM((rows, wide), BF16),
            pltpu.VMEM((rows, 384), BF16),
            pltpu.VMEM((2, rows, 128), BF16),
            pltpu.VMEM((256, 2 * rows), BF16),
            pltpu.VMEM((256, 2 * rows), BF16),
            pltpu.VMEM((1, 4 * rows), F32),
            pltpu.VMEM((1, 4 * rows), F32),
            pltpu.VMEM((128, 4 * rows), F32),
            pltpu.VMEM((rows, wide), F32),
            pltpu.VMEM((rows, wide), BF16),
            pltpu.VMEM((2, rows, inner), F32),
            pltpu.VMEM((rows, inner), BF16),
            pltpu.VMEM((rows, 128), F32),
            dma, dma((count,)), dma, dma((count,)), dma, dma((count,)),
            dma, dma((7,)), dma, dma((4,)), dma, dma((16,)), dma((8,)),
            dma((15,)),
        ],
        compiler_params=pltpu.CompilerParams(
            collective_id=0, has_side_effects=True, vmem_limit_bytes=66 * 1000 * 1000
        ),
        name="layer",
    )(
        residual, queries_a, keys_a, values_a, queries_b, keys_b, values_b, mix_lambda.T, head_gain,
        out_a, out_b, norm_gain.reshape(1, wide), w_gate, w_up, w_down.T,
    )


def solution(mesh):
    in_specs = (
        P("sp", None),
        P("sp", "tp"),
        P("sp", "tp"),
        P("sp", "tp"),
        P("sp", "tp"),
        P("sp", "tp"),
        P("sp", "tp"),
        P(None, "tp"),
        P(),
        P("tp", None),
        P("tp", None),
        P(),
        P("sp", "tp"),
        P("sp", "tp"),
        P("tp", "sp"),
    )
    return jax.shard_map(
        local, mesh=mesh, in_specs=in_specs, out_specs=P("sp", "tp"), check_vma=False
    )
```
